32 devices in a mesh: sp: 16 (over z, y, x), tp: 2 (over core).
Axes of the slice: x: 2, y: 2, z: 4, core: 2. Of those that a mesh axis runs over, the one named last changes fastest.
Arguments:
- value_in: bfloat16 [4096, 2048], P('sp', 'tp'), may hold values from -25 to 25, as said below
- gate_in: bfloat16 [4096, 2048], P('sp', 'tp'), may hold values from -6 to 6
- taps: float32 [31, 2048], P(None, 'tp'), may hold values from -1 to 1
- gain: float32 [2048], P('tp'), may hold values from 0.1 to 1.9
- shift: float32 [2048], P('tp'), may hold values from -3 to 3
- w_out: bfloat16 [2048, 2048], P('tp'), may hold values from -0.125 to 0.125
- grad_out: bfloat16 [4096, 2048], P('sp'), may hold values from -6 to 6
Outputs:
- d_value: bfloat16 [4096, 2048], P('sp', 'tp')
- d_gate: bfloat16 [4096, 2048], P('sp', 'tp')
- d_taps: float32 [31, 2048], P(None, 'tp')
- d_gain: float32 [2048], P('tp')
- d_shift: float32 [2048], P('tp')
The draws below stay inside these ranges and needn't reach their ends.
Inputs may be any that keep to these rules, and one draw needn't show every extreme that they name: `value_in`: channel blocks of different magnitude.
All inputs are finite; a program needn't handle non-finite values.
Results may differ from the reference program's by a relative error of at most 0.007.
Values may be sent and summed in bfloat16 or wider, within the bound.
No kernel may reach another device: no remote copies, remote signals or barrier semaphores. Data moves between devices by JAX's collectives and lax.ppermute only.
A program may use at most 64 MiB of HBM per device.

```python
import math
import jax
import jax.numpy as jnp
from jax import lax

C = 2048
D = 2048
KERNEL = 31
TOK_DEV = 256
TOKENS = 4096
N_SP = 16


def draw_value_in(key, part):
    key_base = jax.random.fold_in(key, 11)
    key_group = jax.random.fold_in(key, 12)
    key_flip = jax.random.fold_in(key, 13)
    base = jnp.clip(jax.random.normal(key_base, (TOKENS, C), jnp.float32), -4.0, 4.0)
    column = jnp.exp(jax.random.uniform(key_group, (C,), jnp.float32, -0.7, 0.7))
    flip = jax.random.randint(key_flip, (), 0, 2)
    upper = (jnp.arange(C) >= C // 2).astype(jnp.int32)
    factor = jnp.where(upper == flip, 3.0, 1.0)
    return (base * column * factor).astype(jnp.bfloat16)


def shard_levels(own_key, extent, pieces, low, high):
    factor_of = 1.0
    for position, shards_of in pieces:
        heights = jax.random.uniform(jax.random.fold_in(jax.random.fold_in(own_key, 6), position), (shards_of,), jnp.float32, low / len(pieces), high / len(pieces))
        factor_of = factor_of * jnp.repeat(jnp.exp(heights), extent[position] // shards_of).reshape((-1,) + (1,) * (len(extent) - 1 - position))
    return factor_of


def noise(rng, extent, scale, most, pieces=(), kind=jnp.bfloat16):
    array = scale * jax.random.normal(rng, extent, jnp.float32)
    if pieces:
        array = array * shard_levels(rng, extent, pieces, -0.22, 0.18)
    return jnp.clip(array, -most, most).astype(kind)


def setup_inputs(seed: int = 0) -> dict:
    splits = jax.random.split(jax.random.key(seed), 8)
    return {
        "value_in": draw_value_in(jax.random.fold_in(splits[7], 71), 0),
        "gate_in": noise(splits[1], (TOKENS, C), 1.5, 6.0, ((0, 16), (1, 2))),
        "taps": noise(splits[2], (KERNEL, C), 0.18, 1.0, ((1, 2),), jnp.float32),
        "gain": jnp.clip(1.0 + 0.18 * jax.random.normal(splits[3], (C,), jnp.float32), 0.1, 1.9),
        "shift": noise(splits[4], (C,), 0.5, 3.0, ((0, 2),), jnp.float32),
        "w_out": noise(splits[5], (C, D), D ** -0.5, 0.125, ((0, 2),)),
        "grad_out": noise(splits[6], (TOKENS, D), 1.0, 6.0, ((0, 16),)),
    }


EPS = 1e-05

def convolve(window, taps, count):
    total = jnp.zeros((count, window.shape[1]), jnp.float32)
    for offset in range(taps.shape[0]):
        total = total + taps[offset] * window[offset:offset + count]
    return total

def norm_backward(conv_out, grad_rows, gain, shift, w_out):
    width = conv_out.shape[1]
    mean = lax.optimization_barrier(jnp.sum(conv_out, 1)) / width
    var = lax.optimization_barrier(jnp.sum(conv_out * conv_out, 1)) / width - mean * mean
    inv = lax.rsqrt(var + EPS)
    normed = (conv_out - mean[:, None]) * inv[:, None]
    pre = normed * gain + shift
    grad_mix = jnp.dot(grad_rows, w_out.T, preferred_element_type=jnp.float32)
    sig = jax.nn.sigmoid(pre)
    grad_pre = grad_mix * sig * (1.0 + pre * (1.0 - sig))
    grad_normed = grad_pre * gain
    first = lax.optimization_barrier(jnp.sum(grad_normed, 1)) / width
    second = lax.optimization_barrier(jnp.sum(grad_normed * normed, 1)) / width
    grad_conv = inv[:, None] * (grad_normed - first[:, None] - normed * second[:, None])
    return (grad_conv, grad_pre, normed)

def reference(value_in, gate_in, taps, gain, shift, w_out, grad_out):
    half = KERNEL // 2
    gate_sig = jax.nn.sigmoid(gate_in.astype(jnp.float32))
    gated = (value_in.astype(jnp.float32) * gate_sig).astype(jnp.bfloat16)
    gated_pad = jnp.pad(gated, ((half, half), (0, 0)))

    def first_pass(index):
        start = (index * TOK_DEV).astype(jnp.int32)
        window = lax.dynamic_slice_in_dim(gated_pad, start, TOK_DEV + 2 * half, 0).astype(jnp.float32)
        conv_out = convolve(window, taps, TOK_DEV)
        grad_rows = lax.dynamic_slice_in_dim(grad_out, start, TOK_DEV, 0)
        grad_conv, grad_pre, normed = norm_backward(conv_out, grad_rows, gain, shift, w_out)
        return (grad_conv, lax.optimization_barrier(jnp.sum(grad_pre * normed, 0)), lax.optimization_barrier(jnp.sum(grad_pre, 0)))
    blocks = jnp.arange(N_SP, dtype=jnp.int32)
    grad_conv, gain_parts, shift_parts = lax.map(first_pass, blocks)
    grad_conv = grad_conv.reshape(TOKENS, C)
    grad_pad = jnp.pad(grad_conv, ((half, half), (0, 0)))

    def second_pass(index):
        start = (index * TOK_DEV).astype(jnp.int32)
        window = lax.dynamic_slice_in_dim(gated_pad, start, TOK_DEV + 2 * half, 0).astype(jnp.float32)
        grad_win = lax.dynamic_slice_in_dim(grad_pad, start, TOK_DEV + 2 * half, 0)
        own = grad_win[half:half + TOK_DEV]
        grad_gated = jnp.zeros((TOK_DEV, C), jnp.float32)
        for offset in range(KERNEL):
            grad_gated = grad_gated + taps[offset] * grad_win[2 * half - offset:2 * half - offset + TOK_DEV]
        tap_terms = jnp.stack([lax.optimization_barrier(jnp.sum(own * window[offset:offset + TOK_DEV], 0)) for offset in range(KERNEL)])
        return (grad_gated, tap_terms)
    grad_gated, tap_parts = lax.map(second_pass, blocks)
    grad_gated = grad_gated.reshape(TOKENS, C)
    scale = 1.0 / math.sqrt(TOKENS)
    d_value = (grad_gated * gate_sig).astype(jnp.bfloat16)
    d_gate = (grad_gated * value_in.astype(jnp.float32) * gate_sig * (1.0 - gate_sig)).astype(jnp.bfloat16)
    d_taps = lax.optimization_barrier(jnp.sum(tap_parts, 0)) * scale
    d_gain = lax.optimization_barrier(jnp.sum(gain_parts, 0)) * scale
    d_shift = lax.optimization_barrier(jnp.sum(shift_parts, 0)) * scale
    return (d_value, d_gate, d_taps, d_gain, d_shift)
```

```python
import functools
import math

import jax
import jax.numpy as jnp
from jax import lax
from jax.experimental import pallas as pl
from jax.experimental.pallas import tpu as pltpu
from jax.sharding import PartitionSpec as P

EPS = 1e-05
LANES = 128
F32 = jnp.float32
BF16 = jnp.bfloat16
EXACT = lax.Precision.HIGHEST
VMEM = pl.BlockSpec(memory_space=pltpu.VMEM)
SMEM = pl.BlockSpec(memory_space=pltpu.SMEM)
HBM = pl.BlockSpec(memory_space=pltpu.HBM)


def up(value, step):
    return -(-value // step) * step


def call(body, name, outs, args, aliases=None, flops=0, specs=None, grid=None, limit=24):
    return pl.pallas_call(
        body,
        name=name,
        out_shape=[jax.ShapeDtypeStruct(shape, dtype) for shape, dtype in outs],
        in_specs=specs if specs else [VMEM] * len(args),
        out_specs=[VMEM] * len(outs),
        input_output_aliases=aliases or {},
        grid=grid or (),
        compiler_params=pltpu.CompilerParams(vmem_limit_bytes=limit * 2**20),
        cost_estimate=pl.CostEstimate(flops=flops, bytes_accessed=0, transcendentals=0),
    )(*args)


def gate_and_mix(
    pad,
    tile,
    flags,
    value_hbm,
    gate_hbm,
    grads_hbm,
    w_hbm,
    gated,
    mix,
    send_even,
    send_odd,
    value,
    gate,
    grads,
    w,
    sems,
):
    rows, channels = value.shape
    first = [
        pltpu.make_async_copy(source, target, sems.at[at])
        for at, (source, target) in enumerate(
            ((gate_hbm, gate), (value_hbm, value), (grads_hbm, grads))
        )
    ]
    weights = [
        pltpu.make_async_copy(
            w_hbm.at[pl.ds(at, tile), :], w.at[pl.ds(at, tile), :], sems.at[3 + at // tile]
        )
        for at in range(0, channels, tile)
    ]
    for copy in first + weights:
        copy.start()
    first[0].wait()
    first[1].wait()
    odd = flags[0] == 1
    for block in range(channels // LANES):
        lanes = slice(block * LANES, (block + 1) * LANES)
        sig = jax.nn.sigmoid(gate[:, lanes].astype(F32))
        product = (value[:, lanes].astype(F32) * sig).astype(BF16)
        gated[block, 2 * pad : 2 * pad + rows, :] = product.astype(F32)
        top = product[: 2 * pad]
        bottom = product[rows - 2 * pad :]
        send_even[: 2 * pad, lanes] = jnp.where(odd, top, bottom)
        send_odd[: 2 * pad, lanes] = jnp.where(odd, bottom, top)
    first[2].wait()
    for index, copy in enumerate(weights):
        copy.wait()
        mixed = lax.dot_general(
            grads[...],
            w[index * tile : (index + 1) * tile, :],
            (((1,), (1,)), ((), ())),
            preferred_element_type=F32,
        )
        for part in range(tile // LANES):
            lanes = slice(part * LANES, (part + 1) * LANES)
            mix[index * (tile // LANES) + part, pad : pad + rows, :] = mixed[:, lanes]
        top = mixed[:pad].astype(BF16)
        bottom = mixed[rows - pad :].astype(BF16)
        lanes = slice(index * tile, (index + 1) * tile)
        send_even[2 * pad :, lanes] = jnp.where(odd, top, bottom)
        send_odd[2 * pad :, lanes] = jnp.where(odd, bottom, top)


def conv_rows(taps, source, block, lanes, first, count, shift):
    total = jnp.zeros((count, LANES), F32)
    for tap in range(taps.shape[0]):
        total = total + taps[pl.ds(tap, 1), lanes] * source[block, pl.ds(first + tap + shift, count), :]
    return total


def pieces(first, last, most):
    count = -(-(last - first) // most)
    size = up(-(-(last - first) // count), 8)
    return [(at, min(size, last - at)) for at in range(first, last, size)]


def conv_inner(pad, gated, taps, out):
    blocks, height, _ = out.shape
    shift = pad - taps.shape[0] // 2

    def body(block, carry):
        lanes = pl.ds(pl.multiple_of(block * LANES, LANES), LANES)
        for at, count in pieces(2 * pad, height - 2 * pad, 56):
            out[block, at : at + count, :] = conv_rows(taps, gated, block, lanes, at, count, shift)
        return carry

    lax.fori_loop(0, blocks, body, 0)


def lane_sums(part):
    ones = jnp.ones((8, LANES), F32)
    return lax.dot_general(
        ones, part, (((1,), (1,)), ((), ())), precision=EXACT, preferred_element_type=F32
    )[0:1]


def spread(line):
    first = (lax.broadcasted_iota(jnp.int32, (8, LANES), 0) == 0).astype(F32)
    rows = jnp.concatenate([line, jnp.zeros((7, line.shape[1]), F32)], 0)
    return lax.dot_general(
        rows, first, (((0,), (0,)), ((), ())), precision=EXACT, preferred_element_type=F32
    )


def conv_edges(
    pad, flags, from_even, from_odd, taps, gated_in, mix_in, conv_in, gated, mix, conv, stats, part
):
    blocks, height, _ = conv.shape
    shift = pad - taps.shape[0] // 2
    odd = flags[0] == 1

    def fill(block, carry):
        lanes = pl.ds(pl.multiple_of(block * LANES, LANES), LANES)
        even_rows = from_even[:, lanes].astype(F32)
        odd_rows = from_odd[:, lanes].astype(F32)
        low = jnp.where(odd, even_rows, odd_rows)
        high = jnp.where(odd, odd_rows, even_rows)
        gated[block, : 2 * pad, :] = low[: 2 * pad]
        gated[block, height :, :] = high[: 2 * pad]
        mix[block, :pad, :] = low[2 * pad :]
        mix[block, height - pad :, :] = high[2 * pad :]
        for at in (0, height - 2 * pad):
            conv[block, at : at + 2 * pad, :] = conv_rows(
                taps, gated, block, lanes, at, 2 * pad, shift
            )
        return carry

    lax.fori_loop(0, blocks, fill, 0)

    def sums(chunk, carry):
        rows = pl.ds(pl.multiple_of(chunk * 16, 16), 16)
        first = jnp.zeros((16, LANES), F32)
        second = jnp.zeros((16, LANES), F32)
        for block in range(blocks):
            value = conv[block, rows, :]
            first = first + value
            second = second + value * value
        part[0, rows, :] = first
        part[1, rows, :] = second
        return carry

    lax.fori_loop(0, height // 16, sums, 0)
    stats[0:1, :] = lane_sums(part[0])
    stats[1:2, :] = lane_sums(part[1])


def moments(mine, other, width):
    mean = (mine[0:1, :] + other[0:1, :]) / width
    var = (mine[1:2, :] + other[1:2, :]) / width - mean * mean
    return mean, lax.rsqrt(var + EPS)


def norm_back(pad, width, conv, mix, stats, stats_other, gain, shift, normed, grad, second, sums, part, line):
    blocks, height, _ = conv.shape
    mean, inv = moments(stats, stats_other, width)
    line[0] = spread(mean)
    line[1] = spread(inv)

    def chunk_rows(rows, keep):
        mean_rows = line[0, rows, :]
        inv_rows = line[1, rows, :]
        first = jnp.zeros((16, LANES), F32)
        other = jnp.zeros((16, LANES), F32)
        kept = []
        for block in range(blocks):
            lanes = slice(block * LANES, (block + 1) * LANES)
            norm = (conv[block, rows, :] - mean_rows) * inv_rows
            gain_row = gain[:, lanes]
            pre = norm * gain_row + shift[:, lanes]
            sig = jax.nn.sigmoid(pre)
            grad_pre = mix[block, rows, :] * sig * (1.0 + pre * (1.0 - sig))
            grad_norm = grad_pre * gain_row
            normed[block, rows, :] = norm
            grad[block, rows, :] = grad_norm
            first = first + grad_norm
            other = other + grad_norm * norm
            if keep:
                product = grad_pre * norm
                kept += [product[:8] + product[8:], grad_pre[:8] + grad_pre[8:]]
        part[0, rows, :] = first
        part[1, rows, :] = other
        return kept

    for at in range(0, pad, 16):
        chunk_rows(pl.ds(at, 16), False)
        chunk_rows(pl.ds(height - pad + at, 16), False)

    def body(chunk, carry):
        kept = chunk_rows(pl.ds(pl.multiple_of(pad + chunk * 16, 16), 16), True)
        return tuple(old + new for old, new in zip(carry, kept))

    zero = tuple(jnp.zeros((8, LANES), F32) for _ in range(2 * blocks))
    totals = lax.fori_loop(0, (height - 2 * pad) // 16, body, zero)
    for block in range(blocks):
        for which in range(2):
            sums[which, block : block + 1, :] = jnp.sum(totals[2 * block + which], 0, keepdims=True)
    second[0:1, :] = lane_sums(part[0])
    second[1:2, :] = lane_sums(part[1])


def tap_sums(
    pad, width, kernel, flags, normed, grad, stats, stats_other, second, second_other, sums, gated, grad_conv, packed, line, raw
):
    blocks, height, _ = normed.shape
    rows = height - 2 * pad
    each = up(kernel + 1, 16)
    shift = pad - kernel // 2
    _, inv = moments(stats, stats_other, width)
    line[0] = spread(inv)
    line[1] = spread((second[0:1, :] + second_other[0:1, :]) / width)
    line[2] = spread((second[1:2, :] + second_other[1:2, :]) / width)
    raw[...] = jnp.zeros_like(raw)

    def finish(block, carry):
        for at, count in pieces(0, height, 48):
            span = slice(at, at + count)
            grad_conv[block, span, :] = line[0, span, :] * (
                grad[block, span, :] - line[1, span, :] - normed[block, span, :] * line[2, span, :]
            )
        return carry

    lax.fori_loop(0, blocks, finish, 0)

    @pl.when(flags[1] == 1)
    def _():
        grad_conv[:, :pad, :] = jnp.zeros((blocks, pad, LANES), F32)

    @pl.when(flags[2] == 1)
    def _():
        grad_conv[:, height - pad :, :] = jnp.zeros((blocks, pad, LANES), F32)

    def body(block, carry):
        base = pl.multiple_of(block * each, each)
        for low in range(0, kernel, 8):
            taps = range(low, min(low + 8, kernel))
            totals = [jnp.zeros((8, LANES), F32) for _ in taps]
            for at in range(0, rows, 32):
                own = grad_conv[block, pad + at : pad + at + 32, :]
                for index, tap in enumerate(taps):
                    term = own * gated[block, pl.ds(pad + at + tap + shift, 32), :]
                    totals[index] = totals[index] + (
                        (term[0:8] + term[8:16]) + (term[16:24] + term[24:32])
                    )
            for index, tap in enumerate(taps):
                raw[pl.ds(base + tap, 1), :] = jnp.sum(totals[index], 0, keepdims=True)
        raw[pl.ds(base + kernel, 1), :] = sums[0, pl.ds(block, 1), :]
        return carry

    lax.fori_loop(0, blocks, body, 0)
    raw[blocks * each : blocks * each + blocks, :] = sums[1]
    packed[...] = raw[...].astype(BF16)


def conv_back(pad, grad_conv, taps, value, gate, d_value, d_gate):
    blocks, height, _ = grad_conv.shape
    rows = height - 2 * pad
    kernel = taps.shape[0]
    top = pad + kernel // 2

    def body(block, carry):
        lanes = pl.ds(pl.multiple_of(block * LANES, LANES), LANES)
        for at, count in pieces(0, rows, 64):
            total = jnp.zeros((count, LANES), F32)
            for tap in range(kernel):
                total = total + taps[pl.ds(tap, 1), lanes] * grad_conv[
                    block, pl.ds(at + top - tap, count), :
                ]
            sig = jax.nn.sigmoid(gate[at : at + count, lanes].astype(F32))
            scaled = total * sig
            d_value[at : at + count, lanes] = scaled.astype(BF16)
            d_gate[at : at + count, lanes] = (
                scaled * value[at : at + count, lanes].astype(F32) * (1.0 - sig)
            ).astype(BF16)
        return carry

    lax.fori_loop(0, blocks, body, 0)


def unpack(scale, kernel, mine, other, d_taps, d_gain, d_shift):
    each = up(kernel + 1, 16)
    blocks = d_gain.shape[0]
    total = (mine[...].astype(F32) + other[...].astype(F32)) * scale
    for block in range(blocks):
        base = block * each
        d_taps[:, block * LANES : (block + 1) * LANES] = total[base : base + kernel]
        d_gain[block : block + 1, :] = total[base + kernel : base + kernel + 1]
    d_shift[...] = total[blocks * each : blocks * each + blocks]


def swap_cores(line):
    count = lax.axis_size("tp")
    if count == 1:
        return jnp.zeros_like(line)
    assert count == 2
    return lax.ppermute(line, "tp", [(0, 1), (1, 0)])


def radices(count):
    found = []
    step = 1
    odd = 3
    while (count // step) % 2 == 0:
        step *= 2
    twos = step
    while step < count:
        while (count // step) % odd == 0:
            found.append((odd, step // twos))
            step *= odd
        odd += 2
    step = count // twos
    while step < count:
        found.append((2, step))
        step *= 2
    return found


def turn(count, radix, step, shift_by):
    pairs = []
    for i in range(count):
        digit = (i // step) % radix
        pairs.append((i, i + ((digit + shift_by) % radix - digit) * step))
    return pairs


def shards(value_in, gate_in, taps, gain, shift, w_out, grad_out):
    kernel, channels = taps.shape
    rows = value_in.shape[0]
    depth = grad_out.shape[1]
    count = lax.axis_size("sp")
    width = channels * lax.axis_size("tp")
    blocks = channels // LANES
    pad = up(kernel // 2 + 1, 16)
    height = rows + 2 * pad
    index = lax.axis_index("sp")
    flags = jnp.stack(
        [index % 2, (index == 0).astype(jnp.int32), (index == count - 1).astype(jnp.int32)]
    ).astype(jnp.int32)
    tile = 2 * LANES if channels % (2 * LANES) == 0 else LANES
    each = up(kernel + 1, 16)

    gated, mix, send_even, send_odd = pl.pallas_call(
        functools.partial(gate_and_mix, pad, tile),
        name="gate_and_mix",
        out_shape=[
            jax.ShapeDtypeStruct((blocks, height + 2 * pad, LANES), F32),
            jax.ShapeDtypeStruct((blocks, height, LANES), F32),
            jax.ShapeDtypeStruct((3 * pad, channels), BF16),
            jax.ShapeDtypeStruct((3 * pad, channels), BF16),
        ],
        in_specs=[SMEM] + [HBM] * 4,
        out_specs=[VMEM] * 4,
        scratch_shapes=[
            pltpu.VMEM((rows, channels), BF16),
            pltpu.VMEM((rows, channels), BF16),
            pltpu.VMEM((rows, depth), BF16),
            pltpu.VMEM((channels, depth), BF16),
            pltpu.SemaphoreType.DMA((3 + channels // tile,)),
        ],
        compiler_params=pltpu.CompilerParams(vmem_limit_bytes=24 * 2**20),
    )(flags, *(pltpu.with_memory_space_constraint(x, pltpu.HBM) for x in (value_in, gate_in, grad_out, w_out)))
    swap_odd = [(i, i + 1) for i in range(1, count - 1, 2)]
    swap_even = [(i, i + 1) for i in range(0, count - 1, 2)]
    from_odd = lax.ppermute(send_odd, "sp", swap_odd + [(b, a) for a, b in swap_odd])
    from_even = lax.ppermute(send_even, "sp", swap_even + [(b, a) for a, b in swap_even])
    conv_flops = 2 * kernel * rows * channels
    (inner,) = call(
        functools.partial(conv_inner, pad),
        "conv_inner",
        [((blocks, height, LANES), F32)],
        (gated, taps),
        flops=conv_flops,
    )
    gated, mix, conv, stats = pl.pallas_call(
        functools.partial(conv_edges, pad),
        name="conv_edges",
        out_shape=[
            jax.ShapeDtypeStruct(gated.shape, F32),
            jax.ShapeDtypeStruct(mix.shape, F32),
            jax.ShapeDtypeStruct(inner.shape, F32),
            jax.ShapeDtypeStruct((2, height), F32),
        ],
        in_specs=[SMEM] + [VMEM] * 6,
        out_specs=[VMEM] * 4,
        input_output_aliases={4: 0, 5: 1, 6: 2},
        scratch_shapes=[pltpu.VMEM((2, height, LANES), F32)],
        compiler_params=pltpu.CompilerParams(vmem_limit_bytes=24 * 2**20),
    )(flags, from_even, from_odd, taps, gated, mix, inner)
    stats_other = swap_cores(stats)
    normed, grad, second, sums = pl.pallas_call(
        functools.partial(norm_back, pad, width),
        name="norm_back",
        out_shape=[
            jax.ShapeDtypeStruct(conv.shape, F32),
            jax.ShapeDtypeStruct(conv.shape, F32),
            jax.ShapeDtypeStruct((2, height), F32),
            jax.ShapeDtypeStruct((2, blocks, LANES), F32),
        ],
        in_specs=[VMEM] * 6,
        out_specs=[VMEM] * 4,
        scratch_shapes=[pltpu.VMEM((2, height, LANES), F32), pltpu.VMEM((2, height, LANES), F32)],
        compiler_params=pltpu.CompilerParams(vmem_limit_bytes=24 * 2**20),
    )(conv, mix, stats, stats_other, gain[None], shift[None])
    second_other = swap_cores(second)
    packed_rows = up(blocks * each + blocks, 16)
    grad_conv, packed = pl.pallas_call(
        functools.partial(tap_sums, pad, width, kernel),
        name="tap_sums",
        out_shape=[
            jax.ShapeDtypeStruct(conv.shape, F32),
            jax.ShapeDtypeStruct((packed_rows, LANES), BF16),
        ],
        in_specs=[SMEM] + [VMEM] * 8,
        out_specs=[VMEM] * 2,
        scratch_shapes=[pltpu.VMEM((3, height, LANES), F32), pltpu.VMEM((packed_rows, LANES), F32)],
        compiler_params=pltpu.CompilerParams(vmem_limit_bytes=24 * 2**20),
    )(flags, normed, grad, stats, stats_other, second, second_other, sums, gated)
    d_value, d_gate = call(
        functools.partial(conv_back, pad),
        "conv_back",
        [((rows, channels), BF16), ((rows, channels), BF16)],
        (grad_conv, taps, value_in, gate_in),
        flops=conv_flops,
    )
    mine = packed
    other = None
    for at, (radix, step) in enumerate(radices(count)):
        digit = (index // step) % radix
        arrived = [
            lax.ppermute(mine, "sp", turn(count, radix, step, shift_by))
            for shift_by in range(1, radix)
        ]
        if radix == 2:
            if step * radix == count:
                other = arrived[0]
                break
            total = mine.astype(F32) + arrived[0].astype(F32)
        else:
            total = jnp.zeros(mine.shape, F32)
            held = [mine] + arrived
            for place in range(radix):
                term = held[0]
                for away in range(1, radix):
                    term = jnp.where((digit - away) % radix == place, held[away], term)
                total = total + term.astype(F32)
        mine = lax.reduce_precision(total, 8, 7).astype(BF16)
    if other is None:
        other = jnp.zeros_like(mine)
    d_taps, d_gain, d_shift = call(
        functools.partial(unpack, 1.0 / math.sqrt(rows * count), kernel),
        "unpack",
        [((kernel, channels), F32), ((blocks, LANES), F32), ((blocks, LANES), F32)],
        (mine, other),
    )
    return (d_value, d_gate, d_taps, d_gain.reshape(channels), d_shift.reshape(channels))


def solution(mesh):
    return jax.shard_map(
        shards,
        mesh=mesh,
        in_specs=(
            P("sp", "tp"),
            P("sp", "tp"),
            P(None, "tp"),
            P("tp"),
            P("tp"),
            P("tp", None),
            P("sp", None),
        ),
        out_specs=(P("sp", "tp"), P("sp", "tp"), P(None, "tp"), P("tp"), P("tp")),
        check_vma=False,
    )
```

```python
import functools
import math

import jax
import jax.numpy as jnp
from jax import lax
from jax.experimental import pallas as pl
from jax.experimental.pallas import tpu as pltpu
from jax.sharding import PartitionSpec as P


EPS = 1e-05
LANES = 128
F32 = jnp.float32
BF16 = jnp.bfloat16
VMEM = pl.BlockSpec(memory_space=pltpu.VMEM)
HBM = pl.BlockSpec(memory_space=pltpu.HBM)


def up(value, step):
    return -(-value // step) * step


def in_hbm(*arrays):
    return [pltpu.with_memory_space_constraint(array, pltpu.HBM) for array in arrays]


def call(body, outs, args, aliases=None, flops=0, specs=None, out_specs=None, scratch=()):
    return pl.pallas_call(
        body,
        out_shape=[jax.ShapeDtypeStruct(shape, dtype) for shape, dtype in outs],
        in_specs=specs if specs else [VMEM] * len(args),
        out_specs=out_specs if out_specs else [VMEM] * len(outs),
        input_output_aliases=aliases or {},
        scratch_shapes=list(scratch),
        compiler_params=pltpu.CompilerParams(vmem_limit_bytes=16 * 2**20),
        cost_estimate=pl.CostEstimate(flops=flops, bytes_accessed=0, transcendentals=0),
    )(*args)


def parity():
    return lax.rem(lax.axis_index("sp"), 2)


def gate_rows(value, gate):
    sig = jax.nn.sigmoid(gate.astype(F32))
    return (value.astype(F32) * sig).astype(BF16)


def edge_rows(pad, value_hbm, gate_hbm, send_even, send_odd, value, gate, sems):
    rows = value_hbm.shape[0]
    odd = parity()
    copies = []
    for at, top in enumerate((odd, 1 - odd)):
        span = pl.ds(pl.multiple_of((1 - top) * (rows - pad), pad), pad)
        copies += [
            pltpu.make_async_copy(value_hbm.at[span, :], value.at[at], sems.at[2 * at]),
            pltpu.make_async_copy(gate_hbm.at[span, :], gate.at[at], sems.at[2 * at + 1]),
        ]
    for copy in copies:
        copy.start()
    for copy in copies:
        copy.wait()
    send_even[...] = gate_rows(value[0], gate[0])
    send_odd[...] = gate_rows(value[1], gate[1])


def gate_and_mix(pad, tile, value, gate, grads, w, gated, mix):
    rows, channels = value.shape
    for index in range(channels // tile):
        if index * tile // LANES < mix.shape[0]:
            mix_rows(tile, index, 0, grads, w, mix)
        for part in range(tile // LANES):
            block = index * (tile // LANES) + part
            lanes = slice(block * LANES, (block + 1) * LANES)
            gated[block, pad : pad + rows, :] = gate_rows(value[:, lanes], gate[:, lanes]).astype(F32)


def mix_rows(tile, index, first, grads, w, mix):
    mixed = lax.dot_general(
        grads[...],
        w[index * tile : (index + 1) * tile, :],
        (((1,), (1,)), ((), ())),
        preferred_element_type=F32,
    )
    for part in range(tile // LANES):
        block = index * (tile // LANES) + part - first
        mix[block] = mixed[:, part * LANES : (part + 1) * LANES]


def mix_rest(tile, first, grads, w, mix):
    for index in range(first * LANES // tile, w.shape[0] // tile):
        mix_rows(tile, index, first, grads, w, mix)


def conv_rows(taps, source, block, lanes, first, count, shift):
    total = jnp.zeros((count, LANES), F32)
    for tap in range(taps.shape[0]):
        total = total + taps[pl.ds(tap, 1), lanes] * source[block, pl.ds(first + tap + shift, count), :]
    return total


def pieces(first, last, most):
    count = -(-(last - first) // most)
    size = up(-(-(last - first) // count), 8)
    return [(at, min(size, last - at)) for at in range(first, last, size)]


def row_sums(conv, part, first, last):
    def sums(chunk, carry):
        rows = pl.ds(pl.multiple_of(first + chunk * 16, 16), 16)
        total = jnp.zeros((16, LANES), F32)
        squares = jnp.zeros((16, LANES), F32)
        for block in range(conv.shape[0]):
            value = conv[block, rows, :]
            total = total + value
            squares = squares + value * value
        part[0, rows, :] = total
        part[1, rows, :] = squares
        return carry

    lax.fori_loop(0, (last - first) // 16, sums, 0)


def conv_inner(pad, gated, taps, out, part):
    blocks, height, _ = out.shape
    shift = pad - taps.shape[0] // 2

    def body(block, carry):
        lanes = pl.ds(pl.multiple_of(block * LANES, LANES), LANES)
        for at, count in pieces(pad, height - pad, 56):
            out[block, at : at + count, :] = conv_rows(taps, gated, block, lanes, at, count, shift)
        return carry

    lax.fori_loop(0, blocks, body, 0)
    row_sums(out, part, pad, height - pad)


def fill_halo(pad, from_even, from_odd, frame, block, lanes):
    rows = frame.shape[1] - 2 * pad
    odd = parity() == 1
    even_rows = from_even[:, lanes].astype(F32)
    odd_rows = from_odd[:, lanes].astype(F32)
    frame[block, :pad, :] = jnp.where(odd, even_rows, odd_rows)
    frame[block, pad + rows :, :] = jnp.where(odd, odd_rows, even_rows)


def thirds(x):
    high = x.astype(BF16).astype(F32)
    middle = (x - high).astype(BF16).astype(F32)
    return high, middle, (x - high) - middle


def lane_sums(first, second):
    stacked = jnp.concatenate([first[...], second[...]], 0)
    split = jnp.concatenate(thirds(stacked), 1).astype(BF16)
    ones = jnp.ones((16, split.shape[1]), BF16)
    return lax.dot_general(
        ones, split, (((1,), (1,)), ((), ())), preferred_element_type=F32
    )[0:1]


def spread(lines):
    rows = [row for line in lines for row in thirds(line)]
    rows += [jnp.zeros_like(lines[0])] * (16 - len(rows))
    shape = (16, len(lines) * LANES)
    part = lax.broadcasted_iota(jnp.int32, shape, 0)
    block = lax.broadcasted_iota(jnp.int32, shape, 1) // LANES
    chosen = jnp.logical_and(part >= 3 * block, part < 3 * block + 3)
    return lax.dot_general(
        jnp.concatenate(rows, 0).astype(BF16),
        chosen.astype(F32).astype(BF16),
        (((0,), (0,)), ((), ())),
        preferred_element_type=F32,
    )


def conv_edges(pad, from_even, from_odd, taps, gated_in, conv_in, part_in, gated, conv, part, stats):
    blocks, height, _ = conv.shape
    shift = pad - taps.shape[0] // 2

    def fill(block, carry):
        lanes = pl.ds(pl.multiple_of(block * LANES, LANES), LANES)
        fill_halo(pad, from_even, from_odd, gated, block, lanes)
        for at in (0, height - pad):
            conv[block, at : at + pad, :] = conv_rows(taps, gated, block, lanes, at, pad, shift)
        return carry

    lax.fori_loop(0, blocks, fill, 0)
    row_sums(conv, part, 0, pad)
    row_sums(conv, part, height - pad, height)
    stats[...] = lane_sums(part[0], part[1])


def moments(mine, other, width):
    total = (mine[...] + other[...]) / width
    rows = total.shape[1] // 2
    mean = total[:, :rows]
    var = total[:, rows:] - mean * mean
    return mean, lax.rsqrt(var + EPS)


def norm_back(
    width,
    at,
    conv,
    mix_low,
    mix_high,
    stats,
    stats_other,
    gain,
    shift,
    normed,
    grad,
    second,
    sums,
    part,
    line,
):
    blocks, height, _ = normed.shape
    half = mix_low.shape[0]
    mean, inv = moments(stats, stats_other, width)
    line[...] = spread([mean[:, at : at + height], inv[:, at : at + height]])

    def body(chunk, carry):
        rows = pl.ds(pl.multiple_of(chunk * 16, 16), 16)
        whole = pl.ds(pl.multiple_of(at + chunk * 16, 16), 16)
        mean_rows = line[rows, :LANES]
        inv_rows = line[rows, LANES:]
        first = jnp.zeros((16, LANES), F32)
        other = jnp.zeros((16, LANES), F32)
        kept = []
        for block in range(blocks):
            lanes = slice(block * LANES, (block + 1) * LANES)
            norm = (conv[block, whole, :] - mean_rows) * inv_rows
            mixed = mix_low[block, whole, :] if block < half else mix_high[block - half, whole, :]
            gain_row = gain[:, lanes]
            pre = norm * gain_row + shift[:, lanes]
            sig = jax.nn.sigmoid(pre)
            grad_pre = mixed * sig * (1.0 + pre * (1.0 - sig))
            grad_norm = grad_pre * gain_row
            normed[block, rows, :] = norm
            grad[block, rows, :] = grad_norm
            first = first + grad_norm
            other = other + grad_norm * norm
            product = grad_pre * norm
            kept += [product[:8] + product[8:], grad_pre[:8] + grad_pre[8:]]
        part[0, rows, :] = first
        part[1, rows, :] = other
        return tuple(old + new for old, new in zip(carry, kept))

    zero = tuple(jnp.zeros((8, LANES), F32) for _ in range(2 * blocks))
    totals = lax.fori_loop(0, height // 16, body, zero)
    for block in range(blocks):
        for which in range(2):
            sums[which, block : block + 1, :] = jnp.sum(totals[2 * block + which], 0, keepdims=True)
    second[...] = lane_sums(part[0], part[1])


def tap_sums(
    pad, width, kernel, at, height, normed, grad, stats, stats_other, second, second_other, gated, *refs
):
    blocks, count, _ = normed.shape
    each = up(kernel + 1, 16)
    shift = pad - kernel // 2
    odd = parity() == 1
    final = at + count == height
    if final:
        sums_low, sums_high, _, raw_in, grad_conv, packed, send_odd, line, raw = refs
    else:
        grad_conv, raw, line = refs
    _, inv = moments(stats, stats_other, width)
    total = (second[...] + second_other[...]) / width
    line[...] = spread([inv[:, at : at + count], total[:, :count], total[:, count:]])
    if not final:
        raw[...] = jnp.zeros_like(raw)

    def body(block, carry):
        for low, size in pieces(0, count, 32):
            span = slice(low, low + size)
            grad_conv[block, pad + at + low : pad + at + low + size, :] = line[span, :LANES] * (
                grad[block, span, :]
                - line[span, LANES : 2 * LANES]
                - normed[block, span, :] * line[span, 2 * LANES :]
            )
        base = pl.multiple_of(block * each, each)
        for low in range(0, kernel, 16):
            taps = range(low, min(low + 16, kernel))
            totals = [jnp.zeros((8, LANES), F32) for _ in taps]
            for row in range(at, at + count, 32):
                own = grad_conv[block, pad + row : pad + row + 32, :]
                for index, tap in enumerate(taps):
                    term = own * gated[block, pl.ds(row + tap + shift, 32), :]
                    totals[index] = totals[index] + (
                        (term[0:8] + term[8:16]) + (term[16:24] + term[24:32])
                    )
            for index, tap in enumerate(taps):
                line_sum = jnp.sum(totals[index], 0, keepdims=True)
                if final:
                    line_sum += raw_in[pl.ds(base + tap, 1), :]
                raw[pl.ds(base + tap, 1), :] = line_sum
        if final:
            one = pl.ds(block, 1)
            raw[pl.ds(base + kernel, 1), :] = sums_low[0, one, :] + sums_high[0, one, :]
            top = grad_conv[block, pad : 2 * pad, :].astype(BF16)
            bottom = grad_conv[block, height : height + pad, :].astype(BF16)
            place = pl.multiple_of(block * pad, pad)
            packed[pl.ds(place + raw.shape[0], pad), :] = jnp.where(odd, top, bottom)
            send_odd[pl.ds(place, pad), :] = jnp.where(odd, bottom, top)
        return carry

    if final:
        raw[blocks * each :, :] = raw_in[blocks * each :, :]
    lax.fori_loop(0, blocks, body, 0)
    if final:
        raw[blocks * each : blocks * each + blocks, :] = sums_low[1] + sums_high[1]
        packed[: raw.shape[0]] = raw[...].astype(BF16)


def fill_back(pad, even, later, odd, frame):
    blocks, height, _ = frame.shape
    base = even.shape[0] - blocks * pad
    upper = parity() == 1
    early = lax.axis_index("tp") == 0

    def fill(block, carry):
        place = pl.multiple_of(block * pad, pad)
        even_rows = jnp.where(
            early, even[pl.ds(place + base, pad), :], later[pl.ds(place + base, pad), :]
        ).astype(F32)
        odd_rows = odd[pl.ds(place, pad), :].astype(F32)
        frame[block, :pad, :] = jnp.where(upper, even_rows, odd_rows)
        frame[block, height - pad :, :] = jnp.where(upper, odd_rows, even_rows)
        return carry

    lax.fori_loop(0, blocks, fill, 0)


def conv_back(pad, stage, spans, before, grad_conv, taps, value, gate, *refs):
    blocks = grad_conv.shape[0]
    kernel = taps.shape[0]
    top = pad + kernel // 2
    sems = refs[-1]
    if stage == 2:
        held_value, held_gate = refs[-3:-1]
        even, later, odd = refs[:3]
        old_value, old_gate = refs[3:5]
        frame, d_value, d_gate = refs[7:10]
        fill_back(pad, even, later, odd, frame)
        grad_conv = frame
    elif stage == 1:
        old_value, old_gate = refs[:2]
        held_value, held_gate, d_value, d_gate = refs[2:6]
    else:
        held_value, held_gate = refs[:2]
    copies = []

    def write(held_pair, which):
        base = 0
        for at, count in which:
            for held, out in zip(held_pair, (d_value, d_gate)):
                copy = pltpu.make_async_copy(
                    held.at[pl.ds(base, count), :],
                    out.at[pl.ds(at, count), :],
                    sems.at[len(copies)],
                )
                copy.start()
                copies.append(copy)
            base += count

    if stage:
        write((old_value, old_gate), before)
    base = 0
    for at, count in spans:
        span = slice(base, base + count)
        base += count

        def body(block, carry):
            lanes = pl.ds(pl.multiple_of(block * LANES, LANES), LANES)
            total = jnp.zeros((count, LANES), F32)
            for tap in range(kernel):
                total = total + taps[pl.ds(tap, 1), lanes] * grad_conv[
                    block, pl.ds(at + top - tap, count), :
                ]
            sig = jax.nn.sigmoid(gate[at : at + count, lanes].astype(F32))
            scaled = total * sig
            held_value[span, lanes] = scaled.astype(BF16)
            held_gate[span, lanes] = (
                scaled * value[at : at + count, lanes].astype(F32) * (1.0 - sig)
            ).astype(BF16)
            return carry

        lax.fori_loop(0, blocks, body, 0)
    if stage == 2:
        write((held_value, held_gate), spans)
    for copy in copies:
        copy.wait()


def merge(summed, mine, other, *refs):
    out = refs[-1]
    rows = summed
    out[:rows] = (mine[:rows].astype(F32) + other[:rows].astype(F32)).astype(BF16)
    if out.shape[0] > rows:
        out[rows:] = mine[rows:]


def unpack(scale, kernel, mine, other, d_taps, d_gain, d_shift):
    each = up(kernel + 1, 16)
    blocks = d_gain.shape[0]
    total = (mine[...].astype(F32) + other[...].astype(F32)) * scale
    for block in range(blocks):
        base = block * each
        d_taps[:, block * LANES : (block + 1) * LANES] = total[base : base + kernel]
        d_gain[block : block + 1, :] = total[base + kernel : base + kernel + 1]
    d_shift[...] = total[blocks * each : blocks * each + blocks]


def swap_cores(line):
    assert lax.axis_size("tp") == 2
    return lax.ppermute(line, "tp", [(0, 1), (1, 0)])


def radices(count):
    twos = []
    odds = []
    step = 1
    while (count // step) % 2 == 0:
        twos.append(step)
        step *= 2
    odd = 3
    while step < count:
        while (count // step) % odd == 0:
            odds.append((odd, step))
            step *= odd
        odd += 2
    return twos, odds


def turn(count, radix, step, shift_by):
    pairs = []
    for i in range(count):
        digit = (i // step) % radix
        pairs.append((i, i + ((digit + shift_by) % radix - digit) * step))
    return pairs


def shards(value_in, gate_in, taps, gain, shift, w_out, grad_out):
    kernel, channels = taps.shape
    rows = value_in.shape[0]
    count = lax.axis_size("sp")
    width = channels * lax.axis_size("tp")
    blocks = channels // LANES
    pad = up(kernel // 2 + 1, 16)
    index = lax.axis_index("sp")
    tile = 2 * LANES if channels % (2 * LANES) == 0 else LANES
    each = up(kernel + 1, 16)
    wide = ((blocks, rows + 2 * pad, LANES), F32)
    frame = ((blocks, rows, LANES), F32)
    lines = ((1, 2 * rows), F32)
    send = ((pad, channels), BF16)
    conv_flops = 2 * kernel * rows * channels
    swap_odd = [(i, i + 1) for i in range(1, count - 1, 2)]
    swap_even = [(i, i + 1) for i in range(0, count - 1, 2)]
    swap_odd += [(b, a) for a, b in swap_odd]
    swap_even += [(b, a) for a, b in swap_even]

    send_even, send_odd = call(
        functools.partial(edge_rows, pad),
        [send, send],
        in_hbm(value_in, gate_in),
        specs=[HBM] * 2,
        scratch=[
            pltpu.VMEM((2, pad, channels), BF16),
            pltpu.VMEM((2, pad, channels), BF16),
            pltpu.SemaphoreType.DMA((4,)),
        ],
        flops=2000 * conv_flops,
    )
    from_odd = lax.ppermute(send_odd, "sp", swap_odd)
    from_even = lax.ppermute(send_even, "sp", swap_even)
    low_blocks = channels // tile // 2 * tile // LANES
    high_blocks = blocks - low_blocks
    gated, mix_low = call(
        functools.partial(gate_and_mix, pad, tile),
        [wide, ((low_blocks, rows, LANES), F32)],
        (value_in, gate_in, grad_out, w_out),
        flops=2 * conv_flops,
    )
    conv, part = call(
        functools.partial(conv_inner, pad),
        [frame, ((2, rows, LANES), F32)],
        (gated, taps),
        flops=conv_flops,
    )
    gated, conv, part, stats = call(
        functools.partial(conv_edges, pad),
        [wide, frame, ((2, rows, LANES), F32), lines],
        (from_even, from_odd, taps, gated, conv, part),
        aliases={3: 0, 4: 1, 5: 2},
        flops=conv_flops,
    )
    stats_other = swap_cores(stats)
    (mix_high,) = call(
        functools.partial(mix_rest, tile, low_blocks),
        [((high_blocks, rows, LANES), F32)],
        (grad_out, w_out),
        flops=conv_flops,
    )
    assert count % 2 == 0
    packed_rows = up(blocks * each + blocks, 16)
    height = up(rows // 2, LANES) if rows > LANES else rows
    halves = [(at, min(height, rows - at)) for at in range(0, rows, height)]
    assert len(halves) == 2
    ready = []
    for at, size in halves:
        normed, grad, second, sums = call(
            functools.partial(norm_back, width, at),
            [((blocks, size, LANES), F32)] * 2 + [((1, 2 * size), F32), ((2, blocks, LANES), F32)],
            (conv, mix_low, mix_high, stats, stats_other, gain[None], shift[None]),
            scratch=[pltpu.VMEM((2, size, LANES), F32), pltpu.VMEM((size, 2 * LANES), F32)],
            flops=conv_flops // 2,
        )
        ready.append((normed, grad, stats, stats_other, second, swap_cores(second), gated, sums))
    (at, size), (next_at, next_size) = halves
    grad_conv, raw = call(
        functools.partial(tap_sums, pad, width, kernel, at, rows),
        [wide, ((packed_rows, LANES), F32)],
        ready[0][:-1],
        scratch=[pltpu.VMEM((size, 3 * LANES), F32)],
        flops=conv_flops // 2,
    )
    grad_conv, packed, send_odd = call(
        functools.partial(tap_sums, pad, width, kernel, next_at, rows),
        [wide, ((packed_rows + blocks * pad, LANES), BF16), ((blocks * pad, LANES), BF16)],
        (*ready[1][:-1], ready[0][-1], ready[1][-1], grad_conv, raw),
        aliases={9: 0},
        scratch=[pltpu.VMEM((next_size, 3 * LANES), F32), pltpu.VMEM((packed_rows, LANES), F32)],
        flops=conv_flops // 2,
    )
    twos, odds = radices(count)
    cores = lax.axis_size("tp")
    orders = [twos, twos[1::-1] + twos[:1:-1]]

    def exchange(at, array):
        pairs = []
        for core in range(cores):
            for a, b in turn(count, 2, orders[core % 2][at], 1):
                pairs.append((a * cores + core, b * cores + core))
        return lax.ppermute(array, ("sp", "tp"), pairs)

    def add(mine, other, height, *after):
        return call(
            functools.partial(merge, packed_rows), [((height, LANES), BF16)], (mine, other, *after)
        )[0]

    first = exchange(0, packed)
    grads_odd = lax.ppermute(send_odd, "sp", swap_odd)

    out = ((rows, channels), BF16)
    middle = up(rows // 2, 16)
    spans = (pieces(pad, middle, 64), pieces(middle, rows - pad, 64))
    edges = [(0, pad), (rows - pad, pad)]
    held = [((sum(n for _, n in part), channels), BF16) for part in (*spans, edges)]
    sources = (grad_conv, taps, value_in, gate_in)
    later, mine = first, packed
    if len(twos) > 1:
        mine = add(packed, first, packed.shape[0])
        later = exchange(1, mine)
    old = call(
        functools.partial(conv_back, pad, 0, spans[0], ()),
        [held[0]] * 2,
        sources,
        scratch=[pltpu.SemaphoreType.DMA((1,))],
        flops=conv_flops // 2,
    )
    *held_rows, d_value, d_gate = call(
        functools.partial(conv_back, pad, 1, spans[1], spans[0]),
        [held[1]] * 2 + [out] * 2,
        (*sources, *old),
        out_specs=[VMEM] * 2 + [HBM] * 2,
        scratch=[pltpu.SemaphoreType.DMA((2 * len(spans[0]),))],
        flops=conv_flops // 2,
    )
    _, d_value, d_gate = call(
        functools.partial(conv_back, pad, 2, edges, spans[1]),
        [wide, out, out],
        (*sources, first, later, grads_odd, *held_rows, d_value, d_gate),
        specs=[VMEM] * 9 + [HBM] * 2,
        out_specs=[VMEM] + [HBM] * 2,
        aliases={0: 0, 9: 1, 10: 2},
        scratch=[pltpu.VMEM(*held[2])] * 2
        + [pltpu.SemaphoreType.DMA((2 * len(spans[1]) + 2 * len(edges),))],
        flops=conv_flops // 8,
    )
    ended = {1: [old[0]], 2: [held_rows[0]]}
    other = later
    for at in range(2, len(twos)):
        mine = add(mine, other, packed_rows, *ended.get(at - 1, []))
        other = exchange(at, mine)
    for radix, step in odds:
        mine = add(mine, other, packed_rows)
        digit = (index // step) % radix
        parts = [mine] + [
            lax.ppermute(mine, "sp", turn(count, radix, step, shift_by))
            for shift_by in range(1, radix)
        ]
        total = jnp.zeros(mine.shape, F32)
        for place in range(radix):
            term = parts[0]
            for away in range(1, radix):
                term = jnp.where((digit - away) % radix == place, parts[away], term)
            total = total + term.astype(F32)
        mine = lax.reduce_precision(total, 8, 7).astype(BF16)
        other = jnp.zeros_like(mine)
    mine, other = mine[:packed_rows], other[:packed_rows]
    d_taps, d_gain, d_shift = call(
        functools.partial(unpack, 1.0 / math.sqrt(rows * count), kernel),
        [((kernel, channels), F32), ((blocks, LANES), F32), ((blocks, LANES), F32)],
        (mine, other),
    )
    return (d_value, d_gate, d_taps, d_gain.reshape(channels), d_shift.reshape(channels))


def solution(mesh):
    return jax.shard_map(
        shards,
        mesh=mesh,
        in_specs=(
            P("sp", "tp"),
            P("sp", "tp"),
            P(None, "tp"),
            P("tp"),
            P("tp"),
            P("tp", None),
            P("sp", None),
        ),
        out_specs=(P("sp", "tp"), P("sp", "tp"), P(None, "tp"), P("tp"), P("tp")),
        check_vma=False,
    )
```

```python
import functools
import math

import jax
import jax.numpy as jnp
from jax import lax
from jax.experimental import pallas as pl
from jax.experimental.pallas import tpu as pltpu
from jax.sharding import PartitionSpec as P


EPS = 1e-05
LANES = 128
F32 = jnp.float32
BF16 = jnp.bfloat16
VMEM = pl.BlockSpec(memory_space=pltpu.VMEM)
HBM = pl.BlockSpec(memory_space=pltpu.HBM)


def up(value, step):
    return -(-value // step) * step


def in_hbm(*arrays):
    return [pltpu.with_memory_space_constraint(array, pltpu.HBM) for array in arrays]


def call(body, outs, args, aliases=None, flops=0, specs=None, out_specs=None, scratch=()):
    return pl.pallas_call(
        body,
        out_shape=[jax.ShapeDtypeStruct(shape, dtype) for shape, dtype in outs],
        in_specs=specs if specs else [VMEM] * len(args),
        out_specs=out_specs if out_specs else [VMEM] * len(outs),
        input_output_aliases=aliases or {},
        scratch_shapes=list(scratch),
        compiler_params=pltpu.CompilerParams(vmem_limit_bytes=16 * 2**20),
        cost_estimate=pl.CostEstimate(flops=flops, bytes_accessed=0, transcendentals=0),
    )(*args)


def parity():
    return lax.rem(lax.axis_index("sp"), 2)


def gate_rows(value, gate):
    sig = jax.nn.sigmoid(gate.astype(F32))
    return (value.astype(F32) * sig).astype(BF16)


def edge_rows(pad, value_hbm, gate_hbm, send_even, send_odd, value, gate, sems):
    rows = value_hbm.shape[0]
    odd = parity()
    copies = []
    for at, top in enumerate((odd, 1 - odd)):
        span = pl.ds(pl.multiple_of((1 - top) * (rows - pad), pad), pad)
        copies += [
            pltpu.make_async_copy(value_hbm.at[span, :], value.at[at], sems.at[2 * at]),
            pltpu.make_async_copy(gate_hbm.at[span, :], gate.at[at], sems.at[2 * at + 1]),
        ]
    for copy in copies:
        copy.start()
    for copy in copies:
        copy.wait()
    send_even[...] = gate_rows(value[0], gate[0])
    send_odd[...] = gate_rows(value[1], gate[1])


def gate_and_mix(pad, tile, value, gate, grads, w, gated, mix):
    rows, channels = value.shape
    for index in range(channels // tile):
        if index * tile // LANES < mix.shape[0]:
            mix_rows(tile, index, 0, grads, w, mix)
        for part in range(tile // LANES):
            block = index * (tile // LANES) + part
            lanes = slice(block * LANES, (block + 1) * LANES)
            gated[block, pad : pad + rows, :] = gate_rows(value[:, lanes], gate[:, lanes]).astype(F32)


def mix_rows(tile, index, first, grads, w, mix):
    mixed = lax.dot_general(
        grads[...],
        w[index * tile : (index + 1) * tile, :],
        (((1,), (1,)), ((), ())),
        preferred_element_type=F32,
    )
    for part in range(tile // LANES):
        block = index * (tile // LANES) + part - first
        mix[block] = mixed[:, part * LANES : (part + 1) * LANES]


def mix_rest(tile, first, grads, w, mix):
    for index in range(first * LANES // tile, w.shape[0] // tile):
        mix_rows(tile, index, first, grads, w, mix)


def conv_rows(taps, source, block, lanes, first, count, shift):
    total = jnp.zeros((count, LANES), F32)
    for tap in range(taps.shape[0]):
        total = total + taps[pl.ds(tap, 1), lanes] * source[block, pl.ds(first + tap + shift, count), :]
    return total


def pieces(first, last, most):
    count = -(-(last - first) // most)
    size = up(-(-(last - first) // count), 8)
    return [(at, min(size, last - at)) for at in range(first, last, size)]


def row_sums(conv, part, first, last):
    def sums(chunk, carry):
        rows = pl.ds(pl.multiple_of(first + chunk * 16, 16), 16)
        total = jnp.zeros((16, LANES), F32)
        squares = jnp.zeros((16, LANES), F32)
        for block in range(conv.shape[0]):
            value = conv[block, rows, :]
            total = total + value
            squares = squares + value * value
        part[0, rows, :] = total
        part[1, rows, :] = squares
        return carry

    lax.fori_loop(0, (last - first) // 16, sums, 0)


def conv_inner(pad, gated, taps, out, part, middle, low_gap, high_gap):
    blocks, height, _ = out.shape
    kernel = taps.shape[0]
    shift = pad - kernel // 2
    rows = height - 2 * pad

    def body(block, carry):
        lanes = pl.ds(pl.multiple_of(block * LANES, LANES), LANES)
        split_rows(gated, block, pad + shift, rows // 2 + kernel // 2, middle, low_gap, high_gap)
        for at, count in pieces(0, rows // 2, 56):
            both, even, odd = (jnp.zeros((count, LANES), F32) for _ in range(3))
            for pair in range(kernel // 2 + 1):
                span = pl.ds(at + pair, count)
                first = taps[pl.ds(2 * pair, 1), lanes]
                even = even + first * low_gap[span, :]
                if 2 * pair + 1 < kernel:
                    second = taps[pl.ds(2 * pair + 1, 1), lanes]
                    odd = odd + second * high_gap[span, :]
                    first = first + second
                both = both + first * middle[span, :]
            out[block, pl.ds(pad + 2 * at, count, stride=2), :] = both + even
            out[block, pl.ds(pad + 2 * at + 1, count, stride=2), :] = both + odd
        return carry

    lax.fori_loop(0, blocks, body, 0)
    row_sums(out, part, pad, height - pad)


def fill_halo(pad, from_even, from_odd, frame, block, lanes):
    rows = frame.shape[1] - 2 * pad
    odd = parity() == 1
    even_rows = from_even[:, lanes].astype(F32)
    odd_rows = from_odd[:, lanes].astype(F32)
    frame[block, :pad, :] = jnp.where(odd, even_rows, odd_rows)
    frame[block, pad + rows :, :] = jnp.where(odd, odd_rows, even_rows)


def thirds(x):
    high = x.astype(BF16).astype(F32)
    middle = (x - high).astype(BF16).astype(F32)
    return high, middle, (x - high) - middle


def lane_sums(first, second):
    split = jnp.concatenate([*thirds(first[...]), *thirds(second[...])], 1).astype(BF16)
    shape = (split.shape[1], LANES)
    late = lax.broadcasted_iota(jnp.int32, shape, 0) >= 3 * LANES
    right = lax.broadcasted_iota(jnp.int32, shape, 1) >= LANES // 2
    chosen = jnp.where(late == right, 1.0, 0.0).astype(BF16)
    return jnp.dot(split, chosen, preferred_element_type=F32)


def spread(pair):
    left = lax.broadcasted_iota(jnp.int32, pair.shape, 1) < LANES // 2
    turned = pltpu.roll(pair, LANES // 2, 1)
    return jnp.where(left, pair, turned), jnp.where(left, turned, pair)


def conv_edges(pad, from_even, from_odd, taps, gated_in, conv_in, part_in, gated, conv, part, stats):
    blocks, height, _ = conv.shape
    shift = pad - taps.shape[0] // 2

    def fill(block, carry):
        lanes = pl.ds(pl.multiple_of(block * LANES, LANES), LANES)
        fill_halo(pad, from_even, from_odd, gated, block, lanes)
        for at in (0, height - pad):
            conv[block, at : at + pad, :] = conv_rows(taps, gated, block, lanes, at, pad, shift)
        return carry

    lax.fori_loop(0, blocks, fill, 0)
    row_sums(conv, part, 0, pad)
    row_sums(conv, part, height - pad, height)
    stats[...] = lane_sums(part[0], part[1])


def moments(mine, other, width, rows):
    mean, square = spread((mine[rows, :] + other[rows, :]) / width)
    return mean, lax.rsqrt(square - mean * mean + EPS)


def norm_back(
    width,
    at,
    conv,
    mix_low,
    mix_high,
    stats,
    stats_other,
    gain,
    shift,
    normed,
    grad,
    second,
    sums,
    part,
    line,
):
    blocks, height, _ = normed.shape
    half = mix_low.shape[0]
    mean, inv = moments(stats, stats_other, width, slice(at, at + height))
    line[:, :LANES] = mean
    line[:, LANES:] = inv

    def body(chunk, carry):
        rows = pl.ds(pl.multiple_of(chunk * 16, 16), 16)
        whole = pl.ds(pl.multiple_of(at + chunk * 16, 16), 16)
        mean_rows = line[rows, :LANES]
        inv_rows = line[rows, LANES:]
        first = jnp.zeros((16, LANES), F32)
        other = jnp.zeros((16, LANES), F32)
        kept = []
        for block in range(blocks):
            lanes = slice(block * LANES, (block + 1) * LANES)
            norm = (conv[block, whole, :] - mean_rows) * inv_rows
            mixed = mix_low[block, whole, :] if block < half else mix_high[block - half, whole, :]
            gain_row = gain[:, lanes]
            pre = norm * gain_row + shift[:, lanes]
            sig = jax.nn.sigmoid(pre)
            grad_pre = mixed * sig * (1.0 + pre * (1.0 - sig))
            grad_norm = grad_pre * gain_row
            normed[block, rows, :] = norm
            grad[block, rows, :] = grad_norm
            first = first + grad_norm
            other = other + grad_norm * norm
            product = grad_pre * norm
            kept += [product[:8] + product[8:], grad_pre[:8] + grad_pre[8:]]
        part[0, rows, :] = first
        part[1, rows, :] = other
        return tuple(old + new for old, new in zip(carry, kept))

    zero = tuple(jnp.zeros((8, LANES), F32) for _ in range(2 * blocks))
    totals = lax.fori_loop(0, height // 16, body, zero)
    for block in range(blocks):
        for which in range(2):
            sums[which, block : block + 1, :] = jnp.sum(totals[2 * block + which], 0, keepdims=True)
    second[...] = lane_sums(part[0], part[1])


def split_rows(source, block, at, count, middle, low_gap, high_gap):
    even = source[block, pl.ds(at, count, stride=2), :]
    odd = source[block, pl.ds(at + 1, count, stride=2), :]
    after = source[block, pl.ds(at + 2, count, stride=2), :]
    middle[:count, :] = odd
    low_gap[:count, :] = even - odd
    high_gap[:count, :] = after - odd


def fold(term):
    return (term[0:8] + term[8:16]) + (term[16:24] + term[24:32])


def tap_sums(
    pad, width, kernel, at, height, normed, grad, stats, stats_other, second, second_other, gated, *refs
):
    blocks, count, _ = normed.shape
    each = up(kernel + 1, 16)
    shift = pad - kernel // 2
    odd = parity() == 1
    final = at + count == height
    if final:
        sums_low, sums_high, _, raw_in, grad_conv, packed, send_odd, line, *split, raw = refs
    else:
        grad_conv, raw, line, *split = refs
    middle, low_gap, high_gap = split
    line[:, :LANES] = moments(stats, stats_other, width, slice(at, at + count))[1]
    means = spread((second[...] + second_other[...]) / width)
    line[:, LANES : 2 * LANES] = means[0]
    line[:, 2 * LANES :] = means[1]

    def body(block, carry):
        for low, size in pieces(0, count, 32):
            span = slice(low, low + size)
            grad_conv[block, pad + at + low : pad + at + low + size, :] = line[span, :LANES] * (
                grad[block, span, :]
                - line[span, LANES : 2 * LANES]
                - normed[block, span, :] * line[span, 2 * LANES :]
            )
        base = pl.multiple_of(block * each, each)
        split_rows(gated, block, at + shift, count // 2 + kernel // 2, middle, low_gap, high_gap)
        for low in range(0, kernel // 2 + 1, 8):
            pairs = range(low, min(low + 8, kernel // 2 + 1))
            both, evens, odds = ([jnp.zeros((8, LANES), F32) for _ in pairs] for _ in range(3))
            for row in range(0, count // 2, 32):
                even = grad_conv[block, pl.ds(pad + at + 2 * row, 32, stride=2), :]
                odd_rows = grad_conv[block, pl.ds(pad + at + 2 * row + 1, 32, stride=2), :]
                together = even + odd_rows
                for index, pair in enumerate(pairs):
                    span = pl.ds(row + pair, 32)
                    both[index] = both[index] + fold(together * middle[span, :])
                    evens[index] = evens[index] + fold(even * low_gap[span, :])
                    if 2 * pair + 1 < kernel:
                        odds[index] = odds[index] + fold(odd_rows * high_gap[span, :])
            for index, pair in enumerate(pairs):
                for tap, total in ((2 * pair, evens[index]), (2 * pair + 1, odds[index])):
                    if tap < kernel:
                        total = both[index] + total
                        tile = pl.ds(pl.multiple_of((base + tap) * 8, 8), 8)
                        if final:
                            total = jnp.sum(total + raw_in[tile, :], 0, keepdims=True)
                            raw[pl.ds(base + tap, 1), :] = total
                        else:
                            raw[tile, :] = total
        if final:
            one = pl.ds(block, 1)
            raw[pl.ds(base + kernel, 1), :] = sums_low[0, one, :] + sums_high[0, one, :]
            top = grad_conv[block, pad : 2 * pad, :].astype(BF16)
            bottom = grad_conv[block, height : height + pad, :].astype(BF16)
            place = pl.multiple_of(block * pad, pad)
            packed[pl.ds(place + raw.shape[0], pad), :] = jnp.where(odd, top, bottom)
            send_odd[pl.ds(place, pad), :] = jnp.where(odd, bottom, top)
        return carry

    if final:
        raw[blocks * each :, :] = jnp.zeros((raw.shape[0] - blocks * each, LANES), F32)
    lax.fori_loop(0, blocks, body, 0)
    if final:
        raw[blocks * each : blocks * each + blocks, :] = sums_low[1] + sums_high[1]
        packed[: raw.shape[0]] = raw[...].astype(BF16)


def fill_back(pad, even, later, odd, frame):
    blocks, height, _ = frame.shape
    base = even.shape[0] - blocks * pad
    upper = parity() == 1
    early = lax.axis_index("tp") == 0

    def fill(block, carry):
        place = pl.multiple_of(block * pad, pad)
        even_rows = jnp.where(
            early, even[pl.ds(place + base, pad), :], later[pl.ds(place + base, pad), :]
        ).astype(F32)
        odd_rows = odd[pl.ds(place, pad), :].astype(F32)
        frame[block, :pad, :] = jnp.where(upper, even_rows, odd_rows)
        frame[block, height - pad :, :] = jnp.where(upper, odd_rows, even_rows)
        return carry

    lax.fori_loop(0, blocks, fill, 0)


def conv_back(pad, stage, spans, before, grad_conv, taps, value, gate, *refs):
    blocks = grad_conv.shape[0]
    kernel = taps.shape[0]
    top = pad + kernel // 2
    sems = refs[-1]
    if stage == 2:
        held_value, held_gate = refs[-3:-1]
        even, later, odd = refs[:3]
        old_value, old_gate = refs[3:5]
        frame, d_value, d_gate = refs[7:10]
        fill_back(pad, even, later, odd, frame)
        grad_conv = frame
    elif stage == 1:
        old_value, old_gate = refs[:2]
        held_value, held_gate, d_value, d_gate = refs[2:6]
    else:
        held_value, held_gate = refs[:2]
    copies = []

    def write(held_pair, which):
        base = 0
        for at, count in which:
            for held, out in zip(held_pair, (d_value, d_gate)):
                copy = pltpu.make_async_copy(
                    held.at[pl.ds(base, count), :],
                    out.at[pl.ds(at, count), :],
                    sems.at[len(copies)],
                )
                copy.start()
                copies.append(copy)
            base += count

    if stage:
        write((old_value, old_gate), before)
    base = 0
    for at, count in spans:
        span = slice(base, base + count)
        base += count

        def body(block, carry):
            lanes = pl.ds(pl.multiple_of(block * LANES, LANES), LANES)
            total = jnp.zeros((count, LANES), F32)
            for tap in range(kernel):
                total = total + taps[pl.ds(tap, 1), lanes] * grad_conv[
                    block, pl.ds(at + top - tap, count), :
                ]
            sig = jax.nn.sigmoid(gate[at : at + count, lanes].astype(F32))
            scaled = total * sig
            held_value[span, lanes] = scaled.astype(BF16)
            held_gate[span, lanes] = (
                scaled * value[at : at + count, lanes].astype(F32) * (1.0 - sig)
            ).astype(BF16)
            return carry

        lax.fori_loop(0, blocks, body, 0)
    if stage == 2:
        write((held_value, held_gate), spans)
    for copy in copies:
        copy.wait()


def merge(summed, mine, other, *refs):
    out = refs[-1]
    rows = summed
    out[:rows] = (mine[:rows].astype(F32) + other[:rows].astype(F32)).astype(BF16)
    if out.shape[0] > rows:
        out[rows:] = mine[rows:]


def unpack(scale, kernel, mine, other, d_taps, d_gain, d_shift):
    each = up(kernel + 1, 16)
    blocks = d_gain.shape[0]
    total = (mine[...].astype(F32) + other[...].astype(F32)) * scale
    for block in range(blocks):
        base = block * each
        d_taps[:, block * LANES : (block + 1) * LANES] = total[base : base + kernel]
        d_gain[block : block + 1, :] = total[base + kernel : base + kernel + 1]
    d_shift[...] = total[blocks * each : blocks * each + blocks]


def swap_cores(line):
    assert lax.axis_size("tp") == 2
    return lax.ppermute(line, "tp", [(0, 1), (1, 0)])


def radices(count):
    twos = []
    odds = []
    step = 1
    while (count // step) % 2 == 0:
        twos.append(step)
        step *= 2
    odd = 3
    while step < count:
        while (count // step) % odd == 0:
            odds.append((odd, step))
            step *= odd
        odd += 2
    return twos, odds


def turn(count, radix, step, shift_by):
    pairs = []
    for i in range(count):
        digit = (i // step) % radix
        pairs.append((i, i + ((digit + shift_by) % radix - digit) * step))
    return pairs


def shards(value_in, gate_in, taps, gain, shift, w_out, grad_out):
    kernel, channels = taps.shape
    rows = value_in.shape[0]
    count = lax.axis_size("sp")
    width = channels * lax.axis_size("tp")
    blocks = channels // LANES
    pad = up(kernel // 2 + 1, 16)
    index = lax.axis_index("sp")
    tile = 2 * LANES if channels % (2 * LANES) == 0 else LANES
    each = up(kernel + 1, 16)
    wide = ((blocks, rows + 2 * pad, LANES), F32)
    frame = ((blocks, rows, LANES), F32)
    lines = ((rows, LANES), F32)
    send = ((pad, channels), BF16)
    conv_flops = 2 * kernel * rows * channels
    swap_odd = [(i, i + 1) for i in range(1, count - 1, 2)]
    swap_even = [(i, i + 1) for i in range(0, count - 1, 2)]
    swap_odd += [(b, a) for a, b in swap_odd]
    swap_even += [(b, a) for a, b in swap_even]

    send_even, send_odd = call(
        functools.partial(edge_rows, pad),
        [send, send],
        in_hbm(value_in, gate_in),
        specs=[HBM] * 2,
        scratch=[
            pltpu.VMEM((2, pad, channels), BF16),
            pltpu.VMEM((2, pad, channels), BF16),
            pltpu.SemaphoreType.DMA((4,)),
        ],
        flops=2000 * conv_flops,
    )
    from_odd = lax.ppermute(send_odd, "sp", swap_odd)
    from_even = lax.ppermute(send_even, "sp", swap_even)
    low_blocks = max(channels // tile // 4, 1) * tile // LANES
    high_blocks = blocks - low_blocks
    gated, mix_low = call(
        functools.partial(gate_and_mix, pad, tile),
        [wide, ((low_blocks, rows, LANES), F32)],
        (value_in, gate_in, grad_out, w_out),
        flops=2 * conv_flops,
    )
    conv, part = call(
        functools.partial(conv_inner, pad),
        [frame, ((2, rows, LANES), F32)],
        (gated, taps),
        scratch=[pltpu.VMEM((up(rows // 2 + kernel // 2, 8), LANES), F32)] * 3,
        flops=conv_flops,
    )
    gated, conv, part, stats = call(
        functools.partial(conv_edges, pad),
        [wide, frame, ((2, rows, LANES), F32), lines],
        (from_even, from_odd, taps, gated, conv, part),
        aliases={3: 0, 4: 1, 5: 2},
        flops=conv_flops,
    )
    stats_other = swap_cores(stats)
    (mix_high,) = call(
        functools.partial(mix_rest, tile, low_blocks),
        [((high_blocks, rows, LANES), F32)],
        (grad_out, w_out),
        flops=conv_flops,
    )
    assert count % 2 == 0
    packed_rows = up(blocks * each + blocks, 16)
    height = up(rows // 2, LANES) if rows > LANES else rows
    halves = [(at, min(height, rows - at)) for at in range(0, rows, height)]
    assert len(halves) == 2 and height % 64 == 0
    gap = pltpu.VMEM((up(rows // 2 + kernel // 2, 8), LANES), F32)
    ready = []
    for at, size in halves:
        normed, grad, second, sums = call(
            functools.partial(norm_back, width, at),
            [((blocks, size, LANES), F32)] * 2 + [((size, LANES), F32), ((2, blocks, LANES), F32)],
            (conv, mix_low, mix_high, stats, stats_other, gain[None], shift[None]),
            scratch=[pltpu.VMEM((2, size, LANES), F32), pltpu.VMEM((size, 2 * LANES), F32)],
            flops=conv_flops // 2,
        )
        ready.append((normed, grad, stats, stats_other, second, swap_cores(second), gated, sums))
    (at, size), (next_at, next_size) = halves
    grad_conv, raw = call(
        functools.partial(tap_sums, pad, width, kernel, at, rows),
        [wide, ((blocks * each * 8, LANES), F32)],
        ready[0][:-1],
        scratch=[pltpu.VMEM((size, 3 * LANES), F32)] + [gap] * 3,
        flops=conv_flops // 2,
    )
    grad_conv, packed, send_odd = call(
        functools.partial(tap_sums, pad, width, kernel, next_at, rows),
        [wide, ((packed_rows + blocks * pad, LANES), BF16), ((blocks * pad, LANES), BF16)],
        (*ready[1][:-1], ready[0][-1], ready[1][-1], grad_conv, raw),
        aliases={9: 0},
        scratch=[pltpu.VMEM((next_size, 3 * LANES), F32)] + [gap] * 3 + [pltpu.VMEM((packed_rows, LANES), F32)],
        flops=conv_flops // 2,
    )
    twos, odds = radices(count)
    cores = lax.axis_size("tp")
    orders = [twos, twos[1::-1] + twos[:1:-1]]

    def exchange(at, array):
        pairs = []
        for core in range(cores):
            for a, b in turn(count, 2, orders[core % 2][at], 1):
                pairs.append((a * cores + core, b * cores + core))
        return lax.ppermute(array, ("sp", "tp"), pairs)

    def add(mine, other, height, *after):
        return call(
            functools.partial(merge, packed_rows), [((height, LANES), BF16)], (mine, other, *after)
        )[0]

    first = exchange(0, packed)
    grads_odd = lax.ppermute(send_odd, "sp", swap_odd)

    out = ((rows, channels), BF16)
    middle = up(rows // 2, 16)
    spans = (pieces(pad, middle, 64), pieces(middle, rows - pad, 64))
    edges = [(0, pad), (rows - pad, pad)]
    held = [((sum(n for _, n in part), channels), BF16) for part in (*spans, edges)]
    sources = (grad_conv, taps, value_in, gate_in)
    later, mine = first, packed
    if len(twos) > 1:
        mine = add(packed, first, packed.shape[0])
        later = exchange(1, mine)
    old = call(
        functools.partial(conv_back, pad, 0, spans[0], ()),
        [held[0]] * 2,
        sources,
        scratch=[pltpu.SemaphoreType.DMA((1,))],
        flops=conv_flops // 2,
    )
    *held_rows, d_value, d_gate = call(
        functools.partial(conv_back, pad, 1, spans[1], spans[0]),
        [held[1]] * 2 + [out] * 2,
        (*sources, *old),
        out_specs=[VMEM] * 2 + [HBM] * 2,
        scratch=[pltpu.SemaphoreType.DMA((2 * len(spans[0]),))],
        flops=conv_flops // 2,
    )
    _, d_value, d_gate = call(
        functools.partial(conv_back, pad, 2, edges, spans[1]),
        [wide, out, out],
        (*sources, first, later, grads_odd, *held_rows, d_value, d_gate),
        specs=[VMEM] * 9 + [HBM] * 2,
        out_specs=[VMEM] + [HBM] * 2,
        aliases={0: 0, 9: 1, 10: 2},
        scratch=[pltpu.VMEM(*held[2])] * 2
        + [pltpu.SemaphoreType.DMA((2 * len(spans[1]) + 2 * len(edges),))],
        flops=conv_flops // 8,
    )
    ended = {1: [old[0]], 2: [held_rows[0]]}
    other = later
    for at in range(2, len(twos)):
        mine = add(mine, other, packed_rows, *ended.get(at - 1, []))
        other = exchange(at, mine)
    for radix, step in odds:
        mine = add(mine, other, packed_rows)
        digit = (index // step) % radix
        parts = [mine] + [
            lax.ppermute(mine, "sp", turn(count, radix, step, shift_by))
            for shift_by in range(1, radix)
        ]
        total = jnp.zeros(mine.shape, F32)
        for place in range(radix):
            term = parts[0]
            for away in range(1, radix):
                term = jnp.where((digit - away) % radix == place, parts[away], term)
            total = total + term.astype(F32)
        mine = lax.reduce_precision(total, 8, 7).astype(BF16)
        other = jnp.zeros_like(mine)
    mine, other = mine[:packed_rows], other[:packed_rows]
    d_taps, d_gain, d_shift = call(
        functools.partial(unpack, 1.0 / math.sqrt(rows * count), kernel),
        [((kernel, channels), F32), ((blocks, LANES), F32), ((blocks, LANES), F32)],
        (mine, other),
    )
    return (d_value, d_gate, d_taps, d_gain.reshape(channels), d_shift.reshape(channels))


def solution(mesh):
    return jax.shard_map(
        shards,
        mesh=mesh,
        in_specs=(
            P("sp", "tp"),
            P("sp", "tp"),
            P(None, "tp"),
            P("tp"),
            P("tp"),
            P("tp", None),
            P("sp", None),
        ),
        out_specs=(P("sp", "tp"), P("sp", "tp"), P(None, "tp"), P("tp"), P("tp")),
        check_vma=False,
    )
```

```python
import functools
import math

import jax
import jax.numpy as jnp
from jax import lax
from jax.experimental import pallas as pl
from jax.experimental.pallas import tpu as pltpu
from jax.sharding import PartitionSpec as P


EPS = 1e-05
LANES = 128
F32 = jnp.float32
BF16 = jnp.bfloat16
VMEM = pl.BlockSpec(memory_space=pltpu.VMEM)
HBM = pl.BlockSpec(memory_space=pltpu.HBM)


def up(value, step):
    return -(-value // step) * step


def in_hbm(*arrays):
    return [pltpu.with_memory_space_constraint(array, pltpu.HBM) for array in arrays]


def call(body, outs, args, aliases=None, flops=0, specs=None, out_specs=None, scratch=()):
    return pl.pallas_call(
        body,
        out_shape=[jax.ShapeDtypeStruct(shape, dtype) for shape, dtype in outs],
        in_specs=specs if specs else [VMEM] * len(args),
        out_specs=out_specs if out_specs else [VMEM] * len(outs),
        input_output_aliases=aliases or {},
        scratch_shapes=list(scratch),
        compiler_params=pltpu.CompilerParams(vmem_limit_bytes=16 * 2**20),
        cost_estimate=pl.CostEstimate(flops=flops, bytes_accessed=0, transcendentals=0),
    )(*args)


def parity():
    return lax.rem(lax.axis_index("sp"), 2)


def gate_rows(value, gate):
    sig = jax.nn.sigmoid(gate.astype(F32))
    return (value.astype(F32) * sig).astype(BF16)


def edge_rows(pad, value_hbm, gate_hbm, send_even, send_odd, value, gate, sems):
    rows = value_hbm.shape[0]
    odd = parity()
    copies = []
    for at, top in enumerate((odd, 1 - odd)):
        span = pl.ds(pl.multiple_of((1 - top) * (rows - pad), pad), pad)
        copies += [
            pltpu.make_async_copy(value_hbm.at[span, :], value.at[at], sems.at[2 * at]),
            pltpu.make_async_copy(gate_hbm.at[span, :], gate.at[at], sems.at[2 * at + 1]),
        ]
    for copy in copies:
        copy.start()
    for copy in copies:
        copy.wait()
    send_even[...] = gate_rows(value[0], gate[0])
    send_odd[...] = gate_rows(value[1], gate[1])


def gate_and_mix(pad, tile, value, gate, grads, w, gated, mix):
    rows, channels = value.shape
    for index in range(channels // tile):
        if index * tile // LANES < mix.shape[0]:
            mix_rows(tile, index, 0, grads, w, mix)
        for part in range(tile // LANES):
            block = index * (tile // LANES) + part
            lanes = slice(block * LANES, (block + 1) * LANES)
            gated[block, pad : pad + rows, :] = gate_rows(value[:, lanes], gate[:, lanes]).astype(F32)


def mix_rows(tile, index, first, grads, w, mix):
    mixed = lax.dot_general(
        grads[...],
        w[index * tile : (index + 1) * tile, :],
        (((1,), (1,)), ((), ())),
        preferred_element_type=F32,
    )
    for part in range(tile // LANES):
        block = index * (tile // LANES) + part - first
        mix[block] = mixed[:, part * LANES : (part + 1) * LANES]


def mix_rest(tile, first, grads, w, mix):
    for index in range(first * LANES // tile, w.shape[0] // tile):
        mix_rows(tile, index, first, grads, w, mix)


def conv_rows(taps, source, block, lanes, first, count, shift):
    total = jnp.zeros((count, LANES), F32)
    for tap in range(taps.shape[0]):
        total = total + taps[pl.ds(tap, 1), lanes] * source[block, pl.ds(first + tap + shift, count), :]
    return total


def pieces(first, last, most):
    count = -(-(last - first) // most)
    size = up(-(-(last - first) // count), 8)
    return [(at, min(size, last - at)) for at in range(first, last, size)]


def row_sums(conv, part, first, last):
    def sums(chunk, carry):
        rows = pl.ds(pl.multiple_of(first + chunk * 16, 16), 16)
        total = jnp.zeros((16, LANES), F32)
        squares = jnp.zeros((16, LANES), F32)
        for block in range(conv.shape[0]):
            value = conv[block, rows, :]
            total = total + value
            squares = squares + value * value
        part[0, rows, :] = total
        part[1, rows, :] = squares
        return carry

    lax.fori_loop(0, (last - first) // 16, sums, 0)


def conv_inner(pad, gated, taps, out, part, middle, low_gap, high_gap):
    blocks, height, _ = out.shape
    kernel = taps.shape[0]
    shift = pad - kernel // 2
    rows = height - 2 * pad

    def body(block, carry):
        lanes = pl.ds(pl.multiple_of(block * LANES, LANES), LANES)
        split_rows(gated, block, pad + shift, rows // 2 + kernel // 2, middle, low_gap, high_gap)
        for at, count in pieces(0, rows // 2, 56):
            both, even, odd = (jnp.zeros((count, LANES), F32) for _ in range(3))
            for pair in range(kernel // 2 + 1):
                span = pl.ds(at + pair, count)
                first = taps[pl.ds(2 * pair, 1), lanes]
                even = even + first * low_gap[span, :]
                if 2 * pair + 1 < kernel:
                    second = taps[pl.ds(2 * pair + 1, 1), lanes]
                    odd = odd + second * high_gap[span, :]
                    first = first + second
                both = both + first * middle[span, :]
            out[block, pl.ds(pad + 2 * at, count, stride=2), :] = both + even
            out[block, pl.ds(pad + 2 * at + 1, count, stride=2), :] = both + odd
        return carry

    lax.fori_loop(0, blocks, body, 0)
    row_sums(out, part, pad, height - pad)


def fill_halo(pad, from_even, from_odd, frame, block, lanes):
    rows = frame.shape[1] - 2 * pad
    odd = parity() == 1
    even_rows = from_even[:, lanes].astype(F32)
    odd_rows = from_odd[:, lanes].astype(F32)
    frame[block, :pad, :] = jnp.where(odd, even_rows, odd_rows)
    frame[block, pad + rows :, :] = jnp.where(odd, odd_rows, even_rows)


def thirds(x):
    high = x.astype(BF16).astype(F32)
    middle = (x - high).astype(BF16).astype(F32)
    return high, middle, (x - high) - middle


def lane_sums(first, second):
    split = jnp.concatenate([*thirds(first[...]), *thirds(second[...])], 1).astype(BF16)
    shape = (split.shape[1], LANES)
    late = lax.broadcasted_iota(jnp.int32, shape, 0) >= 3 * LANES
    right = lax.broadcasted_iota(jnp.int32, shape, 1) >= LANES // 2
    chosen = jnp.where(late == right, 1.0, 0.0).astype(BF16)
    return jnp.dot(split, chosen, preferred_element_type=F32)


def spread(pair):
    left = lax.broadcasted_iota(jnp.int32, pair.shape, 1) < LANES // 2
    turned = pltpu.roll(pair, LANES // 2, 1)
    return jnp.where(left, pair, turned), jnp.where(left, turned, pair)


def conv_edges(pad, from_even, from_odd, taps, gated_in, conv_in, part_in, gated, conv, part, stats):
    blocks, height, _ = conv.shape
    shift = pad - taps.shape[0] // 2

    def fill(block, carry):
        lanes = pl.ds(pl.multiple_of(block * LANES, LANES), LANES)
        fill_halo(pad, from_even, from_odd, gated, block, lanes)
        for at in (0, height - pad):
            conv[block, at : at + pad, :] = conv_rows(taps, gated, block, lanes, at, pad, shift)
        return carry

    lax.fori_loop(0, blocks, fill, 0)
    row_sums(conv, part, 0, pad)
    row_sums(conv, part, height - pad, height)
    stats[...] = lane_sums(part[0], part[1])


def moments(mine, other, width, rows):
    mean, square = spread((mine[rows, :] + other[rows, :]) / width)
    return mean, lax.rsqrt(square - mean * mean + EPS)


def norm_back(
    width,
    at,
    conv,
    mix_low,
    mix_high,
    stats,
    stats_other,
    gain,
    shift,
    normed,
    grad,
    second,
    sums,
    part,
    line,
):
    blocks, height, _ = normed.shape
    half = mix_low.shape[0]
    mean, inv = moments(stats, stats_other, width, slice(at, at + height))
    line[:, :LANES] = mean
    line[:, LANES:] = inv

    def body(chunk, carry):
        rows = pl.ds(pl.multiple_of(chunk * 32, 32), 32)
        whole = pl.ds(pl.multiple_of(at + chunk * 32, 32), 32)
        mean_rows = line[rows, :LANES]
        inv_rows = line[rows, LANES:]
        first = jnp.zeros((32, LANES), F32)
        other = jnp.zeros((32, LANES), F32)
        kept = []
        for block in range(blocks):
            lanes = slice(block * LANES, (block + 1) * LANES)
            norm = (conv[block, whole, :] - mean_rows) * inv_rows
            mixed = mix_low[block, whole, :] if block < half else mix_high[block - half, whole, :]
            gain_row = gain[:, lanes]
            pre = norm * gain_row + shift[:, lanes]
            sig = jax.nn.sigmoid(pre)
            grad_pre = mixed * sig * (1.0 + pre * (1.0 - sig))
            grad_norm = grad_pre * gain_row
            normed[block, rows, :] = norm
            grad[block, rows, :] = grad_norm
            first = first + grad_norm
            other = other + grad_norm * norm
            product = grad_pre * norm
            kept += [fold(product), fold(grad_pre)]
        part[0, rows, :] = first
        part[1, rows, :] = other
        return tuple(old + new for old, new in zip(carry, kept))

    zero = tuple(jnp.zeros((8, LANES), F32) for _ in range(2 * blocks))
    totals = lax.fori_loop(0, height // 32, body, zero)
    for block in range(blocks):
        for which in range(2):
            sums[which, block : block + 1, :] = jnp.sum(totals[2 * block + which], 0, keepdims=True)
    second[...] = lane_sums(part[0], part[1])


def split_rows(source, block, at, count, middle, low_gap, high_gap):
    even = source[block, pl.ds(at, count, stride=2), :]
    odd = source[block, pl.ds(at + 1, count, stride=2), :]
    after = source[block, pl.ds(at + 2, count, stride=2), :]
    middle[:count, :] = odd
    low_gap[:count, :] = even - odd
    high_gap[:count, :] = after - odd


def fold(term):
    return (term[0:8] + term[8:16]) + (term[16:24] + term[24:32])


def fold_two(first, second):
    top = lax.broadcasted_iota(jnp.int32, first.shape, 0) < 4
    total = jnp.where(top, first, second) + pltpu.roll(jnp.where(top, second, first), 4, 0)
    total = total + pltpu.roll(total, 2, 0)
    return total + pltpu.roll(total, 1, 0)


def tap_sums(
    pad, width, kernel, at, height, normed, grad, stats, stats_other, second, second_other, gated, *refs
):
    blocks, count, _ = normed.shape
    each = up(kernel + 1, 16)
    shift = pad - kernel // 2
    odd = parity() == 1
    final = at + count == height
    if final:
        sums_low, sums_high, _, raw_in, grad_conv, packed, send_odd, line, *split, raw = refs
    else:
        grad_conv, raw, line, *split = refs
    middle, low_gap, high_gap = split
    line[:, :LANES] = moments(stats, stats_other, width, slice(at, at + count))[1]
    means = spread((second[...] + second_other[...]) / width)
    line[:, LANES : 2 * LANES] = means[0]
    line[:, 2 * LANES :] = means[1]

    def body(block, carry):
        for low, size in pieces(0, count, 32):
            span = slice(low, low + size)
            grad_conv[block, pad + at + low : pad + at + low + size, :] = line[span, :LANES] * (
                grad[block, span, :]
                - line[span, LANES : 2 * LANES]
                - normed[block, span, :] * line[span, 2 * LANES :]
            )
        base = pl.multiple_of(block * each, each)
        split_rows(gated, block, at + shift, count // 2 + kernel // 2, middle, low_gap, high_gap)
        for low in range(0, kernel // 2 + 1, 8):
            pairs = range(low, min(low + 8, kernel // 2 + 1))
            both, evens, odds = ([jnp.zeros((8, LANES), F32) for _ in pairs] for _ in range(3))
            for row in range(0, count // 2, 32):
                even = grad_conv[block, pl.ds(pad + at + 2 * row, 32, stride=2), :]
                odd_rows = grad_conv[block, pl.ds(pad + at + 2 * row + 1, 32, stride=2), :]
                together = even + odd_rows
                for index, pair in enumerate(pairs):
                    span = pl.ds(row + pair, 32)
                    both[index] = both[index] + fold(together * middle[span, :])
                    evens[index] = evens[index] + fold(even * low_gap[span, :])
                    if 2 * pair + 1 < kernel:
                        odds[index] = odds[index] + fold(odd_rows * high_gap[span, :])
            for index, pair in enumerate(pairs):
                tiles = [both[index] + evens[index], both[index] + odds[index]]
                for which, tile in enumerate(tiles[: kernel - 2 * pair]):
                    place = pl.ds(pl.multiple_of((base + 2 * pair + which) * 8, 8), 8)
                    if final:
                        tiles[which] = tile + raw_in[place, :]
                    else:
                        raw[place, :] = tile
                if final:
                    halves = fold_two(*tiles)
                    for which in range(min(2, kernel - 2 * pair)):
                        row = halves[4 * which + 3 : 4 * which + 4]
                        raw[pl.ds(base + 2 * pair + which, 1), :] = row
        if final:
            one = pl.ds(block, 1)
            raw[pl.ds(base + kernel, 1), :] = sums_low[0, one, :] + sums_high[0, one, :]
            top = grad_conv[block, pad : 2 * pad, :].astype(BF16)
            bottom = grad_conv[block, height : height + pad, :].astype(BF16)
            place = pl.multiple_of(block * pad, pad)
            packed[pl.ds(place + raw.shape[0], pad), :] = jnp.where(odd, top, bottom)
            send_odd[pl.ds(place, pad), :] = jnp.where(odd, bottom, top)
        return carry

    if final:
        raw[blocks * each :, :] = jnp.zeros((raw.shape[0] - blocks * each, LANES), F32)
    lax.fori_loop(0, blocks, body, 0)
    if final:
        raw[blocks * each : blocks * each + blocks, :] = sums_low[1] + sums_high[1]
        packed[: raw.shape[0]] = raw[...].astype(BF16)


def fill_back(pad, even, later, odd, frame):
    blocks, height, _ = frame.shape
    base = even.shape[0] - blocks * pad
    upper = parity() == 1
    early = lax.axis_index("tp") == 0

    def fill(block, carry):
        place = pl.multiple_of(block * pad, pad)
        even_rows = jnp.where(
            early, even[pl.ds(place + base, pad), :], later[pl.ds(place + base, pad), :]
        ).astype(F32)
        odd_rows = odd[pl.ds(place, pad), :].astype(F32)
        frame[block, :pad, :] = jnp.where(upper, even_rows, odd_rows)
        frame[block, height - pad :, :] = jnp.where(upper, odd_rows, even_rows)
        return carry

    lax.fori_loop(0, blocks, fill, 0)


def conv_back(pad, stage, spans, before, grad_conv, taps, value, gate, *refs):
    blocks = grad_conv.shape[0]
    kernel = taps.shape[0]
    top = pad + kernel // 2
    sems = refs[-1]
    if stage == 2:
        held_value, held_gate = refs[-3:-1]
        even, later, odd = refs[:3]
        old_value, old_gate = refs[3:5]
        frame, d_value, d_gate = refs[7:10]
        fill_back(pad, even, later, odd, frame)
        grad_conv = frame
    elif stage == 1:
        old_value, old_gate = refs[:2]
        held_value, held_gate, d_value, d_gate = refs[2:6]
    else:
        held_value, held_gate = refs[:2]
    copies = []

    def write(held_pair, which):
        base = 0
        for at, count in which:
            for held, out in zip(held_pair, (d_value, d_gate)):
                copy = pltpu.make_async_copy(
                    held.at[pl.ds(base, count), :],
                    out.at[pl.ds(at, count), :],
                    sems.at[len(copies)],
                )
                copy.start()
                copies.append(copy)
            base += count

    if stage:
        write((old_value, old_gate), before)
    base = 0
    for at, count in spans:
        span = slice(base, base + count)
        base += count

        def body(block, carry):
            lanes = pl.ds(pl.multiple_of(block * LANES, LANES), LANES)
            total = jnp.zeros((count, LANES), F32)
            for tap in range(kernel):
                total = total + taps[pl.ds(tap, 1), lanes] * grad_conv[
                    block, pl.ds(at + top - tap, count), :
                ]
            sig = jax.nn.sigmoid(gate[at : at + count, lanes].astype(F32))
            scaled = total * sig
            held_value[span, lanes] = scaled.astype(BF16)
            held_gate[span, lanes] = (
                scaled * value[at : at + count, lanes].astype(F32) * (1.0 - sig)
            ).astype(BF16)
            return carry

        lax.fori_loop(0, blocks, body, 0)
    if stage == 2:
        write((held_value, held_gate), spans)
    for copy in copies:
        copy.wait()


def merge(summed, mine, other, *refs):
    out = refs[-1]
    rows = summed
    out[:rows] = (mine[:rows].astype(F32) + other[:rows].astype(F32)).astype(BF16)
    if out.shape[0] > rows:
        out[rows:] = mine[rows:]


def unpack(scale, kernel, mine, other, d_taps, d_gain, d_shift):
    each = up(kernel + 1, 16)
    blocks = d_gain.shape[0]
    total = (mine[...].astype(F32) + other[...].astype(F32)) * scale
    for block in range(blocks):
        base = block * each
        d_taps[:, block * LANES : (block + 1) * LANES] = total[base : base + kernel]
        d_gain[block : block + 1, :] = total[base + kernel : base + kernel + 1]
    d_shift[...] = total[blocks * each : blocks * each + blocks]


def swap_cores(line):
    assert lax.axis_size("tp") == 2
    return lax.ppermute(line, "tp", [(0, 1), (1, 0)])


def radices(count):
    twos = []
    odds = []
    step = 1
    while (count // step) % 2 == 0:
        twos.append(step)
        step *= 2
    odd = 3
    while step < count:
        while (count // step) % odd == 0:
            odds.append((odd, step))
            step *= odd
        odd += 2
    return twos, odds


def turn(count, radix, step, shift_by):
    pairs = []
    for i in range(count):
        digit = (i // step) % radix
        pairs.append((i, i + ((digit + shift_by) % radix - digit) * step))
    return pairs


def shards(value_in, gate_in, taps, gain, shift, w_out, grad_out):
    kernel, channels = taps.shape
    rows = value_in.shape[0]
    count = lax.axis_size("sp")
    width = channels * lax.axis_size("tp")
    blocks = channels // LANES
    pad = up(kernel // 2 + 1, 16)
    index = lax.axis_index("sp")
    tile = 2 * LANES if channels % (2 * LANES) == 0 else LANES
    each = up(kernel + 1, 16)
    wide = ((blocks, rows + 2 * pad, LANES), F32)
    frame = ((blocks, rows, LANES), F32)
    lines = ((rows, LANES), F32)
    send = ((pad, channels), BF16)
    conv_flops = 2 * kernel * rows * channels
    swap_odd = [(i, i + 1) for i in range(1, count - 1, 2)]
    swap_even = [(i, i + 1) for i in range(0, count - 1, 2)]
    swap_odd += [(b, a) for a, b in swap_odd]
    swap_even += [(b, a) for a, b in swap_even]

    send_even, send_odd = call(
        functools.partial(edge_rows, pad),
        [send, send],
        in_hbm(value_in, gate_in),
        specs=[HBM] * 2,
        scratch=[
            pltpu.VMEM((2, pad, channels), BF16),
            pltpu.VMEM((2, pad, channels), BF16),
            pltpu.SemaphoreType.DMA((4,)),
        ],
        flops=2000 * conv_flops,
    )
    from_odd = lax.ppermute(send_odd, "sp", swap_odd)
    from_even = lax.ppermute(send_even, "sp", swap_even)
    low_blocks = max(channels // tile // 4, 1) * tile // LANES
    high_blocks = blocks - low_blocks
    gated, mix_low = call(
        functools.partial(gate_and_mix, pad, tile),
        [wide, ((low_blocks, rows, LANES), F32)],
        (value_in, gate_in, grad_out, w_out),
        flops=2 * conv_flops,
    )
    conv, part = call(
        functools.partial(conv_inner, pad),
        [frame, ((2, rows, LANES), F32)],
        (gated, taps),
        scratch=[pltpu.VMEM((up(rows // 2 + kernel // 2, 8), LANES), F32)] * 3,
        flops=conv_flops,
    )
    gated, conv, part, stats = call(
        functools.partial(conv_edges, pad),
        [wide, frame, ((2, rows, LANES), F32), lines],
        (from_even, from_odd, taps, gated, conv, part),
        aliases={3: 0, 4: 1, 5: 2},
        flops=conv_flops,
    )
    stats_other = swap_cores(stats)
    (mix_high,) = call(
        functools.partial(mix_rest, tile, low_blocks),
        [((high_blocks, rows, LANES), F32)],
        (grad_out, w_out),
        flops=conv_flops,
    )
    assert count % 2 == 0
    packed_rows = up(blocks * each + blocks, 16)
    height = up(rows // 2, LANES) if rows > LANES else rows
    halves = [(at, min(height, rows - at)) for at in range(0, rows, height)]
    assert len(halves) == 2 and height % 64 == 0
    gap = pltpu.VMEM((up(rows // 2 + kernel // 2, 8), LANES), F32)
    ready = []
    for at, size in halves:
        normed, grad, second, sums = call(
            functools.partial(norm_back, width, at),
            [((blocks, size, LANES), F32)] * 2 + [((size, LANES), F32), ((2, blocks, LANES), F32)],
            (conv, mix_low, mix_high, stats, stats_other, gain[None], shift[None]),
            scratch=[pltpu.VMEM((2, size, LANES), F32), pltpu.VMEM((size, 2 * LANES), F32)],
            flops=conv_flops // 2,
        )
        ready.append((normed, grad, stats, stats_other, second, swap_cores(second), gated, sums))
    (at, size), (next_at, next_size) = halves
    grad_conv, raw = call(
        functools.partial(tap_sums, pad, width, kernel, at, rows),
        [wide, ((blocks * each * 8, LANES), F32)],
        ready[0][:-1],
        scratch=[pltpu.VMEM((size, 3 * LANES), F32)] + [gap] * 3,
        flops=conv_flops // 2,
    )
    grad_conv, packed, send_odd = call(
        functools.partial(tap_sums, pad, width, kernel, next_at, rows),
        [wide, ((packed_rows + blocks * pad, LANES), BF16), ((blocks * pad, LANES), BF16)],
        (*ready[1][:-1], ready[0][-1], ready[1][-1], grad_conv, raw),
        aliases={9: 0},
        scratch=[pltpu.VMEM((next_size, 3 * LANES), F32)] + [gap] * 3 + [pltpu.VMEM((packed_rows, LANES), F32)],
        flops=conv_flops // 2,
    )
    twos, odds = radices(count)
    cores = lax.axis_size("tp")
    orders = [twos, twos[1::-1] + twos[:1:-1]]

    def exchange(at, array):
        pairs = []
        for core in range(cores):
            for a, b in turn(count, 2, orders[core % 2][at], 1):
                pairs.append((a * cores + core, b * cores + core))
        return lax.ppermute(array, ("sp", "tp"), pairs)

    def add(mine, other, height, *after):
        return call(
            functools.partial(merge, packed_rows), [((height, LANES), BF16)], (mine, other, *after)
        )[0]

    first = exchange(0, packed)
    grads_odd = lax.ppermute(send_odd, "sp", swap_odd)

    out = ((rows, channels), BF16)
    middle = up(rows // 2, 16)
    spans = (pieces(pad, middle, 64), pieces(middle, rows - pad, 64))
    edges = [(0, pad), (rows - pad, pad)]
    held = [((sum(n for _, n in part), channels), BF16) for part in (*spans, edges)]
    sources = (grad_conv, taps, value_in, gate_in)
    later, mine = first, packed
    if len(twos) > 1:
        mine = add(packed, first, packed.shape[0])
        later = exchange(1, mine)
    old = call(
        functools.partial(conv_back, pad, 0, spans[0], ()),
        [held[0]] * 2,
        sources,
        scratch=[pltpu.SemaphoreType.DMA((1,))],
        flops=conv_flops // 2,
    )
    *held_rows, d_value, d_gate = call(
        functools.partial(conv_back, pad, 1, spans[1], spans[0]),
        [held[1]] * 2 + [out] * 2,
        (*sources, *old),
        out_specs=[VMEM] * 2 + [HBM] * 2,
        scratch=[pltpu.SemaphoreType.DMA((2 * len(spans[0]),))],
        flops=conv_flops // 2,
    )
    _, d_value, d_gate = call(
        functools.partial(conv_back, pad, 2, edges, spans[1]),
        [wide, out, out],
        (*sources, first, later, grads_odd, *held_rows, d_value, d_gate),
        specs=[VMEM] * 9 + [HBM] * 2,
        out_specs=[VMEM] + [HBM] * 2,
        aliases={0: 0, 9: 1, 10: 2},
        scratch=[pltpu.VMEM(*held[2])] * 2
        + [pltpu.SemaphoreType.DMA((2 * len(spans[1]) + 2 * len(edges),))],
        flops=conv_flops // 8,
    )
    ended = {1: [old[0]], 2: [held_rows[0]]}
    other = later
    for at in range(2, len(twos)):
        mine = add(mine, other, packed_rows, *ended.get(at - 1, []))
        other = exchange(at, mine)
    for radix, step in odds:
        mine = add(mine, other, packed_rows)
        digit = (index // step) % radix
        parts = [mine] + [
            lax.ppermute(mine, "sp", turn(count, radix, step, shift_by))
            for shift_by in range(1, radix)
        ]
        total = jnp.zeros(mine.shape, F32)
        for place in range(radix):
            term = parts[0]
            for away in range(1, radix):
                term = jnp.where((digit - away) % radix == place, parts[away], term)
            total = total + term.astype(F32)
        mine = lax.reduce_precision(total, 8, 7).astype(BF16)
        other = jnp.zeros_like(mine)
    mine, other = mine[:packed_rows], other[:packed_rows]
    d_taps, d_gain, d_shift = call(
        functools.partial(unpack, 1.0 / math.sqrt(rows * count), kernel),
        [((kernel, channels), F32), ((blocks, LANES), F32), ((blocks, LANES), F32)],
        (mine, other),
    )
    return (d_value, d_gate, d_taps, d_gain.reshape(channels), d_shift.reshape(channels))


def solution(mesh):
    return jax.shard_map(
        shards,
        mesh=mesh,
        in_specs=(
            P("sp", "tp"),
            P("sp", "tp"),
            P(None, "tp"),
            P("tp"),
            P("tp"),
            P("tp", None),
            P("sp", None),
        ),
        out_specs=(P("sp", "tp"), P("sp", "tp"), P(None, "tp"), P("tp"), P("tp")),
        check_vma=False,
    )
```

```python
import functools
import math

import jax
import jax.numpy as jnp
from jax import lax
from jax.experimental import pallas as pl
from jax.experimental.pallas import tpu as pltpu
from jax.sharding import PartitionSpec as P


EPS = 1e-05
LANES = 128
F32 = jnp.float32
BF16 = jnp.bfloat16
VMEM = pl.BlockSpec(memory_space=pltpu.VMEM)
HBM = pl.BlockSpec(memory_space=pltpu.HBM)


def up(value, step):
    return -(-value // step) * step


def in_hbm(*arrays):
    return [pltpu.with_memory_space_constraint(array, pltpu.HBM) for array in arrays]


def call(body, outs, args, aliases=None, flops=0, specs=None, out_specs=None, scratch=()):
    return pl.pallas_call(
        body,
        out_shape=[jax.ShapeDtypeStruct(shape, dtype) for shape, dtype in outs],
        in_specs=specs if specs else [VMEM] * len(args),
        out_specs=out_specs if out_specs else [VMEM] * len(outs),
        input_output_aliases=aliases or {},
        scratch_shapes=list(scratch),
        compiler_params=pltpu.CompilerParams(vmem_limit_bytes=16 * 2**20),
        cost_estimate=pl.CostEstimate(flops=flops, bytes_accessed=0, transcendentals=0),
    )(*args)


def parity():
    return lax.rem(lax.axis_index("sp"), 2)


def gate_rows(value, gate):
    sig = jax.nn.sigmoid(gate.astype(F32))
    return (value.astype(F32) * sig).astype(BF16)


def edge_rows(pad, value_hbm, gate_hbm, send_even, send_odd, value, gate, sems):
    rows = value_hbm.shape[0]
    odd = parity()
    copies = []
    for at, top in enumerate((odd, 1 - odd)):
        span = pl.ds(pl.multiple_of((1 - top) * (rows - pad), pad), pad)
        copies += [
            pltpu.make_async_copy(value_hbm.at[span, :], value.at[at], sems.at[2 * at]),
            pltpu.make_async_copy(gate_hbm.at[span, :], gate.at[at], sems.at[2 * at + 1]),
        ]
    for copy in copies:
        copy.start()
    for copy in copies:
        copy.wait()
    send_even[...] = gate_rows(value[0], gate[0])
    send_odd[...] = gate_rows(value[1], gate[1])


def gate_and_mix(pad, tile, value, gate, grads, w, gated, mix):
    rows, channels = value.shape
    for index in range(channels // tile):
        if index * tile // LANES < mix.shape[0]:
            mix_rows(tile, index, 0, grads, w, mix)
        for part in range(tile // LANES):
            block = index * (tile // LANES) + part
            lanes = slice(block * LANES, (block + 1) * LANES)
            gated[block, pad : pad + rows, :] = gate_rows(value[:, lanes], gate[:, lanes]).astype(F32)


def mix_rows(tile, index, first, grads, w, mix):
    mixed = lax.dot_general(
        grads[...],
        w[index * tile : (index + 1) * tile, :],
        (((1,), (1,)), ((), ())),
        preferred_element_type=F32,
    )
    for part in range(tile // LANES):
        block = index * (tile // LANES) + part - first
        mix[block] = mixed[:, part * LANES : (part + 1) * LANES]


def mix_rest(tile, first, grads, w, mix):
    for index in range(first * LANES // tile, w.shape[0] // tile):
        mix_rows(tile, index, first, grads, w, mix)


def conv_rows(taps, source, block, lanes, first, count, shift):
    total = jnp.zeros((count, LANES), F32)
    for tap in range(taps.shape[0]):
        total = total + taps[pl.ds(tap, 1), lanes] * source[block, pl.ds(first + tap + shift, count), :]
    return total


def pieces(first, last, most):
    count = -(-(last - first) // most)
    size = up(-(-(last - first) // count), 8)
    return [(at, min(size, last - at)) for at in range(first, last, size)]


def row_sums(conv, part, first, last):
    def sums(chunk, carry):
        rows = pl.ds(pl.multiple_of(first + chunk * 16, 16), 16)
        total = jnp.zeros((16, LANES), F32)
        squares = jnp.zeros((16, LANES), F32)
        for block in range(conv.shape[0]):
            value = conv[block, rows, :]
            total = total + value
            squares = squares + value * value
        part[0, rows, :] = total
        part[1, rows, :] = squares
        return carry

    lax.fori_loop(0, (last - first) // 16, sums, 0)


def conv_inner(pad, gated, taps, out, part, middle, low_gap, high_gap):
    blocks, height, _ = out.shape
    kernel = taps.shape[0]
    shift = pad - kernel // 2
    rows = height - 2 * pad

    def body(block, carry):
        lanes = pl.ds(pl.multiple_of(block * LANES, LANES), LANES)
        split_rows(gated, block, pad + shift, rows // 2 + kernel // 2, middle, low_gap, high_gap)
        for at, count in pieces(0, rows // 2, 56):
            both, even, odd = (jnp.zeros((count, LANES), F32) for _ in range(3))
            for pair in range(kernel // 2 + 1):
                span = pl.ds(at + pair, count)
                first = taps[pl.ds(2 * pair, 1), lanes]
                even = even + first * low_gap[span, :]
                if 2 * pair + 1 < kernel:
                    second = taps[pl.ds(2 * pair + 1, 1), lanes]
                    odd = odd + second * high_gap[span, :]
                    first = first + second
                both = both + first * middle[span, :]
            out[block, pl.ds(pad + 2 * at, count, stride=2), :] = both + even
            out[block, pl.ds(pad + 2 * at + 1, count, stride=2), :] = both + odd
        return carry

    lax.fori_loop(0, blocks, body, 0)
    row_sums(out, part, pad, height - pad)


def fill_halo(pad, from_even, from_odd, frame, block, lanes):
    rows = frame.shape[1] - 2 * pad
    odd = parity() == 1
    even_rows = from_even[:, lanes].astype(F32)
    odd_rows = from_odd[:, lanes].astype(F32)
    frame[block, :pad, :] = jnp.where(odd, even_rows, odd_rows)
    frame[block, pad + rows :, :] = jnp.where(odd, odd_rows, even_rows)


def thirds(x):
    high = x.astype(BF16).astype(F32)
    middle = (x - high).astype(BF16).astype(F32)
    return high, middle, (x - high) - middle


def lane_sums(first, second):
    split = jnp.concatenate([*thirds(first[...]), *thirds(second[...])], 1).astype(BF16)
    shape = (split.shape[1], LANES)
    late = lax.broadcasted_iota(jnp.int32, shape, 0) >= 3 * LANES
    right = lax.broadcasted_iota(jnp.int32, shape, 1) >= LANES // 2
    chosen = jnp.where(late == right, 1.0, 0.0).astype(BF16)
    return jnp.dot(split, chosen, preferred_element_type=F32)


def spread(pair):
    left = lax.broadcasted_iota(jnp.int32, pair.shape, 1) < LANES // 2
    turned = pltpu.roll(pair, LANES // 2, 1)
    return jnp.where(left, pair, turned), jnp.where(left, turned, pair)


def conv_edges(pad, from_even, from_odd, taps, gated_in, conv_in, part_in, gated, conv, part, stats):
    blocks, height, _ = conv.shape
    shift = pad - taps.shape[0] // 2

    def fill(block, carry):
        lanes = pl.ds(pl.multiple_of(block * LANES, LANES), LANES)
        fill_halo(pad, from_even, from_odd, gated, block, lanes)
        for at in (0, height - pad):
            conv[block, at : at + pad, :] = conv_rows(taps, gated, block, lanes, at, pad, shift)
        return carry

    lax.fori_loop(0, blocks, fill, 0)
    row_sums(conv, part, 0, pad)
    row_sums(conv, part, height - pad, height)
    stats[...] = lane_sums(part[0], part[1])


def moments(mine, other, width, rows):
    mean, square = spread((mine[rows, :] + other[rows, :]) / width)
    return mean, lax.rsqrt(square - mean * mean + EPS)


def norm_back(
    width,
    at,
    conv,
    mix_low,
    mix_high,
    stats,
    stats_other,
    gain,
    shift,
    normed,
    grad,
    second,
    sums,
    part,
    line,
):
    blocks, height, _ = normed.shape
    half = mix_low.shape[0]
    mean, inv = moments(stats, stats_other, width, slice(at, at + height))
    line[:, :LANES] = mean
    line[:, LANES:] = inv

    def body(chunk, carry):
        rows = pl.ds(pl.multiple_of(chunk * 32, 32), 32)
        whole = pl.ds(pl.multiple_of(at + chunk * 32, 32), 32)
        mean_rows = line[rows, :LANES]
        inv_rows = line[rows, LANES:]
        first = jnp.zeros((32, LANES), F32)
        other = jnp.zeros((32, LANES), F32)
        kept = []
        for block in range(blocks):
            lanes = slice(block * LANES, (block + 1) * LANES)
            norm = (conv[block, whole, :] - mean_rows) * inv_rows
            mixed = mix_low[block, whole, :] if block < half else mix_high[block - half, whole, :]
            gain_row = gain[:, lanes]
            pre = norm * gain_row + shift[:, lanes]
            sig = jax.nn.sigmoid(pre)
            grad_pre = mixed * sig * (1.0 + pre * (1.0 - sig))
            grad_norm = grad_pre * gain_row
            normed[block, rows, :] = norm
            grad[block, rows, :] = grad_norm
            first = first + grad_norm
            other = other + grad_norm * norm
            product = grad_pre * norm
            kept += [fold(product), fold(grad_pre)]
        part[0, rows, :] = first
        part[1, rows, :] = other
        return tuple(old + new for old, new in zip(carry, kept))

    zero = tuple(jnp.zeros((8, LANES), F32) for _ in range(2 * blocks))
    totals = lax.fori_loop(0, height // 32, body, zero)
    for block in range(blocks):
        for which in range(2):
            sums[which, block : block + 1, :] = jnp.sum(totals[2 * block + which], 0, keepdims=True)
    second[...] = lane_sums(part[0], part[1])


def split_rows(source, block, at, count, middle, low_gap, high_gap):
    even = source[block, pl.ds(at, count, stride=2), :]
    odd = source[block, pl.ds(at + 1, count, stride=2), :]
    after = source[block, pl.ds(at + 2, count, stride=2), :]
    middle[:count, :] = odd
    low_gap[:count, :] = even - odd
    high_gap[:count, :] = after - odd


def fold(term):
    return (term[0:8] + term[8:16]) + (term[16:24] + term[24:32])


def tap_sums(
    pad, width, kernel, at, height, normed, grad, stats, stats_other, second, second_other, gated, *refs
):
    blocks, count, _ = normed.shape
    each = up(kernel + 1, 16)
    shift = pad - kernel // 2
    odd = parity() == 1
    final = at + count == height
    if final:
        sums_low, sums_high, _, raw_in, grad_conv, packed, send_odd, line, *split, raw = refs
    else:
        grad_conv, raw, line, *split = refs
    middle, low_gap, high_gap = split
    line[:, :LANES] = moments(stats, stats_other, width, slice(at, at + count))[1]
    means = spread((second[...] + second_other[...]) / width)
    line[:, LANES : 2 * LANES] = means[0]
    line[:, 2 * LANES :] = means[1]

    def body(block, carry):
        for low, size in pieces(0, count, 32):
            span = slice(low, low + size)
            grad_conv[block, pad + at + low : pad + at + low + size, :] = line[span, :LANES] * (
                grad[block, span, :]
                - line[span, LANES : 2 * LANES]
                - normed[block, span, :] * line[span, 2 * LANES :]
            )
        base = pl.multiple_of(block * each, each)
        split_rows(gated, block, at + shift, count // 2 + kernel // 2, middle, low_gap, high_gap)
        for low in range(0, kernel // 2 + 1, 8):
            pairs = range(low, min(low + 8, kernel // 2 + 1))
            both, evens, odds = ([jnp.zeros((8, LANES), F32) for _ in pairs] for _ in range(3))
            for row in range(0, count // 2, 32):
                even = grad_conv[block, pl.ds(pad + at + 2 * row, 32, stride=2), :]
                odd_rows = grad_conv[block, pl.ds(pad + at + 2 * row + 1, 32, stride=2), :]
                together = even + odd_rows
                for index, pair in enumerate(pairs):
                    span = pl.ds(row + pair, 32)
                    both[index] = both[index] + fold(together * middle[span, :])
                    evens[index] = evens[index] + fold(even * low_gap[span, :])
                    if 2 * pair + 1 < kernel:
                        odds[index] = odds[index] + fold(odd_rows * high_gap[span, :])
            for index, pair in enumerate(pairs):
                for tap, total in ((2 * pair, evens[index]), (2 * pair + 1, odds[index])):
                    if tap < kernel:
                        total = both[index] + total
                        tile = pl.ds(pl.multiple_of((base + tap) * 8, 8), 8)
                        if final:
                            total = jnp.sum(total + raw_in[tile, :], 0, keepdims=True)
                            raw[pl.ds(base + tap, 1), :] = total
                        else:
                            raw[tile, :] = total
        if final:
            one = pl.ds(block, 1)
            raw[pl.ds(base + kernel, 1), :] = sums_low[0, one, :] + sums_high[0, one, :]
            top = grad_conv[block, pad : 2 * pad, :].astype(BF16)
            bottom = grad_conv[block, height : height + pad, :].astype(BF16)
            place = pl.multiple_of(block * pad, pad)
            packed[pl.ds(place + raw.shape[0], pad), :] = jnp.where(odd, top, bottom)
            send_odd[pl.ds(place, pad), :] = jnp.where(odd, bottom, top)
        return carry

    if final:
        raw[blocks * each :, :] = jnp.zeros((raw.shape[0] - blocks * each, LANES), F32)
    lax.fori_loop(0, blocks, body, 0)
    if final:
        raw[blocks * each : blocks * each + blocks, :] = sums_low[1] + sums_high[1]
        packed[: raw.shape[0]] = raw[...].astype(BF16)


def fill_back(pad, even, later, odd, frame):
    blocks, height, _ = frame.shape
    base = even.shape[0] - blocks * pad
    upper = parity() == 1
    early = lax.axis_index("tp") == 0

    def fill(block, carry):
        place = pl.multiple_of(block * pad, pad)
        even_rows = jnp.where(
            early, even[pl.ds(place + base, pad), :], later[pl.ds(place + base, pad), :]
        ).astype(F32)
        odd_rows = odd[pl.ds(place, pad), :].astype(F32)
        frame[block, :pad, :] = jnp.where(upper, even_rows, odd_rows)
        frame[block, height - pad :, :] = jnp.where(upper, odd_rows, even_rows)
        return carry

    lax.fori_loop(0, blocks, fill, 0)


def conv_back(pad, stage, spans, before, grad_conv, taps, value, gate, *refs):
    blocks = grad_conv.shape[0]
    kernel = taps.shape[0]
    top = pad + kernel // 2
    sems = refs[-1]
    if stage == 2:
        held_value, held_gate = refs[-3:-1]
        even, later, odd = refs[:3]
        old_value, old_gate = refs[3:5]
        frame, d_value, d_gate = refs[7:10]
        fill_back(pad, even, later, odd, frame)
        grad_conv = frame
    elif stage == 1:
        old_value, old_gate = refs[:2]
        held_value, held_gate, d_value, d_gate = refs[2:6]
    else:
        held_value, held_gate = refs[:2]
    copies = []

    def write(held_pair, which):
        base = 0
        for at, count in which:
            for held, out in zip(held_pair, (d_value, d_gate)):
                copy = pltpu.make_async_copy(
                    held.at[pl.ds(base, count), :],
                    out.at[pl.ds(at, count), :],
                    sems.at[len(copies)],
                )
                copy.start()
                copies.append(copy)
            base += count

    if stage:
        write((old_value, old_gate), before)
    base = 0
    for at, count in spans:
        span = slice(base, base + count)
        base += count

        def body(block, carry):
            lanes = pl.ds(pl.multiple_of(block * LANES, LANES), LANES)
            total = jnp.zeros((count, LANES), F32)
            for tap in range(kernel):
                total = total + taps[pl.ds(tap, 1), lanes] * grad_conv[
                    block, pl.ds(at + top - tap, count), :
                ]
            sig = jax.nn.sigmoid(gate[at : at + count, lanes].astype(F32))
            scaled = total * sig
            held_value[span, lanes] = scaled.astype(BF16)
            held_gate[span, lanes] = (
                scaled * value[at : at + count, lanes].astype(F32) * (1.0 - sig)
            ).astype(BF16)
            return carry

        lax.fori_loop(0, blocks, body, 0)
    if stage == 2:
        write((held_value, held_gate), spans)
    for copy in copies:
        copy.wait()


def merge(summed, mine, other, *refs):
    out = refs[-1]
    rows = summed
    out[:rows] = (mine[:rows].astype(F32) + other[:rows].astype(F32)).astype(BF16)
    if out.shape[0] > rows:
        out[rows:] = mine[rows:]


def unpack(scale, kernel, mine, other, d_taps, d_gain, d_shift):
    each = up(kernel + 1, 16)
    blocks = d_gain.shape[0]
    total = (mine[...].astype(F32) + other[...].astype(F32)) * scale
    for block in range(blocks):
        base = block * each
        d_taps[:, block * LANES : (block + 1) * LANES] = total[base : base + kernel]
        d_gain[block : block + 1, :] = total[base + kernel : base + kernel + 1]
    d_shift[...] = total[blocks * each : blocks * each + blocks]


def swap_cores(line):
    assert lax.axis_size("tp") == 2
    return lax.ppermute(line, "tp", [(0, 1), (1, 0)])


def radices(count):
    twos = []
    odds = []
    step = 1
    while (count // step) % 2 == 0:
        twos.append(step)
        step *= 2
    odd = 3
    while step < count:
        while (count // step) % odd == 0:
            odds.append((odd, step))
            step *= odd
        odd += 2
    return twos, odds


def turn(count, radix, step, shift_by):
    pairs = []
    for i in range(count):
        digit = (i // step) % radix
        pairs.append((i, i + ((digit + shift_by) % radix - digit) * step))
    return pairs


def shards(value_in, gate_in, taps, gain, shift, w_out, grad_out):
    kernel, channels = taps.shape
    rows = value_in.shape[0]
    count = lax.axis_size("sp")
    width = channels * lax.axis_size("tp")
    blocks = channels // LANES
    pad = up(kernel // 2 + 1, 16)
    index = lax.axis_index("sp")
    tile = 2 * LANES if channels % (2 * LANES) == 0 else LANES
    each = up(kernel + 1, 16)
    wide = ((blocks, rows + 2 * pad, LANES), F32)
    frame = ((blocks, rows, LANES), F32)
    lines = ((rows, LANES), F32)
    send = ((pad, channels), BF16)
    conv_flops = 2 * kernel * rows * channels
    swap_odd = [(i, i + 1) for i in range(1, count - 1, 2)]
    swap_even = [(i, i + 1) for i in range(0, count - 1, 2)]
    swap_odd += [(b, a) for a, b in swap_odd]
    swap_even += [(b, a) for a, b in swap_even]

    send_even, send_odd = call(
        functools.partial(edge_rows, pad),
        [send, send],
        in_hbm(value_in, gate_in),
        specs=[HBM] * 2,
        scratch=[
            pltpu.VMEM((2, pad, channels), BF16),
            pltpu.VMEM((2, pad, channels), BF16),
            pltpu.SemaphoreType.DMA((4,)),
        ],
        flops=2000 * conv_flops,
    )
    from_odd = lax.ppermute(send_odd, "sp", swap_odd)
    from_even = lax.ppermute(send_even, "sp", swap_even)
    low_blocks = max(channels // tile // 4, 1) * tile // LANES
    high_blocks = blocks - low_blocks
    gated, mix_low = call(
        functools.partial(gate_and_mix, pad, tile),
        [wide, ((low_blocks, rows, LANES), F32)],
        (value_in, gate_in, grad_out, w_out),
        flops=2 * conv_flops,
    )
    conv, part = call(
        functools.partial(conv_inner, pad),
        [frame, ((2, rows, LANES), F32)],
        (gated, taps),
        scratch=[pltpu.VMEM((up(rows // 2 + kernel // 2, 8), LANES), F32)] * 3,
        flops=conv_flops,
    )
    gated, conv, part, stats = call(
        functools.partial(conv_edges, pad),
        [wide, frame, ((2, rows, LANES), F32), lines],
        (from_even, from_odd, taps, gated, conv, part),
        aliases={3: 0, 4: 1, 5: 2},
        flops=conv_flops,
    )
    stats_other = swap_cores(stats)
    (mix_high,) = call(
        functools.partial(mix_rest, tile, low_blocks),
        [((high_blocks, rows, LANES), F32)],
        (grad_out, w_out),
        flops=conv_flops,
    )
    assert count % 2 == 0
    packed_rows = up(blocks * each + blocks, 16)
    height = up(rows // 2, LANES) if rows > LANES else rows
    halves = [(at, min(height, rows - at)) for at in range(0, rows, height)]
    assert len(halves) == 2 and height % 64 == 0
    gap = pltpu.VMEM((up(rows // 2 + kernel // 2, 8), LANES), F32)
    ready = []
    for at, size in halves:
        normed, grad, second, sums = call(
            functools.partial(norm_back, width, at),
            [((blocks, size, LANES), F32)] * 2 + [((size, LANES), F32), ((2, blocks, LANES), F32)],
            (conv, mix_low, mix_high, stats, stats_other, gain[None], shift[None]),
            scratch=[pltpu.VMEM((2, size, LANES), F32), pltpu.VMEM((size, 2 * LANES), F32)],
            flops=conv_flops // 2,
        )
        ready.append((normed, grad, stats, stats_other, second, swap_cores(second), gated, sums))
    (at, size), (next_at, next_size) = halves
    grad_conv, raw = call(
        functools.partial(tap_sums, pad, width, kernel, at, rows),
        [wide, ((blocks * each * 8, LANES), F32)],
        ready[0][:-1],
        scratch=[pltpu.VMEM((size, 3 * LANES), F32)] + [gap] * 3,
        flops=conv_flops // 2,
    )
    grad_conv, packed, send_odd = call(
        functools.partial(tap_sums, pad, width, kernel, next_at, rows),
        [wide, ((packed_rows + blocks * pad, LANES), BF16), ((blocks * pad, LANES), BF16)],
        (*ready[1][:-1], ready[0][-1], ready[1][-1], grad_conv, raw),
        aliases={9: 0},
        scratch=[pltpu.VMEM((next_size, 3 * LANES), F32)] + [gap] * 3 + [pltpu.VMEM((packed_rows, LANES), F32)],
        flops=conv_flops // 2,
    )
    twos, odds = radices(count)
    cores = lax.axis_size("tp")
    order = twos[:1] + twos[1:3][::-1] + twos[3:]
    turned = [step for at in range(0, len(order), 2) for step in order[at : at + 2][::-1]]
    orders = [order, turned]

    def exchange(at, array):
        pairs = []
        for core in range(cores):
            for a, b in turn(count, 2, orders[core % 2][at], 1):
                pairs.append((a * cores + core, b * cores + core))
        return lax.ppermute(array, ("sp", "tp"), pairs)

    def add(mine, other, height, *after):
        return call(
            functools.partial(merge, packed_rows), [((height, LANES), BF16)], (mine, other, *after)
        )[0]

    first = exchange(0, packed)
    grads_odd = lax.ppermute(send_odd, "sp", swap_odd)

    out = ((rows, channels), BF16)
    middle = up(rows // 2, 16)
    spans = (pieces(pad, middle, 64), pieces(middle, rows - pad, 64))
    edges = [(0, pad), (rows - pad, pad)]
    held = [((sum(n for _, n in part), channels), BF16) for part in (*spans, edges)]
    sources = (grad_conv, taps, value_in, gate_in)
    later, mine = first, packed
    if len(twos) > 1:
        mine = add(packed, first, packed.shape[0])
        later = exchange(1, mine)
    old = call(
        functools.partial(conv_back, pad, 0, spans[0], ()),
        [held[0]] * 2,
        sources,
        scratch=[pltpu.SemaphoreType.DMA((1,))],
        flops=conv_flops // 2,
    )
    *held_rows, d_value, d_gate = call(
        functools.partial(conv_back, pad, 1, spans[1], spans[0]),
        [held[1]] * 2 + [out] * 2,
        (*sources, *old),
        out_specs=[VMEM] * 2 + [HBM] * 2,
        scratch=[pltpu.SemaphoreType.DMA((2 * len(spans[0]),))],
        flops=conv_flops // 2,
    )
    _, d_value, d_gate = call(
        functools.partial(conv_back, pad, 2, edges, spans[1]),
        [wide, out, out],
        (*sources, first, later, grads_odd, *held_rows, d_value, d_gate),
        specs=[VMEM] * 9 + [HBM] * 2,
        out_specs=[VMEM] + [HBM] * 2,
        aliases={0: 0, 9: 1, 10: 2},
        scratch=[pltpu.VMEM(*held[2])] * 2
        + [pltpu.SemaphoreType.DMA((2 * len(spans[1]) + 2 * len(edges),))],
        flops=conv_flops // 8,
    )
    ended = {1: [old[0]], 2: [held_rows[0]]}
    other = later
    for at in range(2, len(twos)):
        mine = add(mine, other, packed_rows, *ended.get(at - 1, []))
        other = exchange(at, mine)
    for radix, step in odds:
        mine = add(mine, other, packed_rows)
        digit = (index // step) % radix
        parts = [mine] + [
            lax.ppermute(mine, "sp", turn(count, radix, step, shift_by))
            for shift_by in range(1, radix)
        ]
        total = jnp.zeros(mine.shape, F32)
        for place in range(radix):
            term = parts[0]
            for away in range(1, radix):
                term = jnp.where((digit - away) % radix == place, parts[away], term)
            total = total + term.astype(F32)
        mine = lax.reduce_precision(total, 8, 7).astype(BF16)
        other = jnp.zeros_like(mine)
    mine, other = mine[:packed_rows], other[:packed_rows]
    d_taps, d_gain, d_shift = call(
        functools.partial(unpack, 1.0 / math.sqrt(rows * count), kernel),
        [((kernel, channels), F32), ((blocks, LANES), F32), ((blocks, LANES), F32)],
        (mine, other),
    )
    return (d_value, d_gate, d_taps, d_gain.reshape(channels), d_shift.reshape(channels))


def solution(mesh):
    return jax.shard_map(
        shards,
        mesh=mesh,
        in_specs=(
            P("sp", "tp"),
            P("sp", "tp"),
            P(None, "tp"),
            P("tp"),
            P("tp"),
            P("tp", None),
            P("sp", None),
        ),
        out_specs=(P("sp", "tp"), P("sp", "tp"), P(None, "tp"), P("tp"), P("tp")),
        check_vma=False,
    )
```
